512 devices in a mesh: rep: 2 (over z_hi), fs: 32 (over z_lo, y), tp: 8 (over x, core).
Axes of the slice: x: 4, y: 8, z: 8 (z_hi: 2, z_lo: 4; z = z_hi * 4 + z_lo), core: 2. Of those that a mesh axis runs over, the one named last changes fastest.
Arguments:
- resid: bfloat16 [16384, 2048], P(('rep', 'fs'), 'tp'), may hold values from -6 to 6
- norm_gains: float32 [3, 2048], replicated, may hold values from 0.1 to 1.9
- gate_one: bfloat16 [2048, 5632], P('fs', 'tp'), may hold values from -0.125 to 0.125
- up_one: bfloat16 [2048, 5632], P('fs', 'tp'), may hold values from -0.125 to 0.125
- down_one: bfloat16 [5632, 2048], P('tp', 'fs'), may hold values from -0.15625 to 0.15625
- proj_u: bfloat16 [2048, 1024], P('fs', 'tp'), may hold values from -0.125 to 0.125
- proj_v: bfloat16 [2048, 1024], P('fs', 'tp'), may hold values from -0.125 to 0.125
- spatial: bfloat16 [8, 128, 128], P('tp'), may hold values from -0.5 to 0.5
- spatial_bias: float32 [8, 128], P('tp'), may hold values from 0.1 to 1.9
- mix_gain: float32 [1024], P('tp'), may hold values from 0.1 to 1.9
- head_gain: float32 [1024], P('tp'), may hold values from 0.1 to 1.9
- proj_out: bfloat16 [1024, 2048], P('tp', 'fs'), may hold values from -0.375 to 0.375
- gate_two: bfloat16 [2048, 5632], P('fs', 'tp'), may hold values from -0.125 to 0.125
- up_two: bfloat16 [2048, 5632], P('fs', 'tp'), may hold values from -0.125 to 0.125
- down_two: bfloat16 [5632, 2048], P('tp', 'fs'), may hold values from -0.15625 to 0.15625
Outputs:
- layer_out: bfloat16 [16384, 2048], P(('rep', 'fs'), 'tp')
The draws below stay inside these ranges and needn't reach their ends.
All inputs are finite; a program needn't handle non-finite values.
Results may differ from the reference program's by a relative error of at most 0.019.
Values may be sent and summed in bfloat16 or wider, within the bound.
A program may use at most 64 MiB of HBM per device.

```python
import jax
import jax.numpy as jnp
from jax import lax

D = 2048
FF = 5632
HEADS = 8
HEAD_DIM = 128
BLOCK = 128
SPAN = 64
GM = 1024
TOKENS = 16384
N_TP = 8


def raised(entries, stream_key, source, target, shards_of, factor):
    owner, partner = [(jnp.arange(entries.shape[position]) // (entries.shape[position] // shards_of)).reshape([-1 if axis == position else 1 for axis in range(entries.ndim)]) for position in (source, target)]
    chosen = jax.random.permutation(stream_key, shards_of)[partner]
    strong = (owner == chosen) | (owner == (partner + shards_of // 2) % shards_of)
    return jnp.where(strong, factor * entries, entries)


def steps_of(own_key, shape, pieces, low, largest):
    def one(dim, shards_of):
        draws = jax.random.uniform(jax.random.fold_in(jax.random.fold_in(own_key, 6), dim), (shards_of,), jnp.float32, low / len(pieces), largest / len(pieces))
        return jnp.repeat(jnp.exp(draws), shape[dim] // shards_of).reshape((-1,) + (1,) * (len(shape) - dim - 1))

    factor_of = one(*pieces[0])
    for cut in pieces[1:]:
        factor_of = factor_of * one(*cut)
    return factor_of


def centred(rng, shape, deviation, reach, cuts=(), held_as=jnp.bfloat16):
    level = steps_of(rng, shape, cuts, -0.22, 0.18) if cuts else 1.0
    drawn = jax.random.normal(rng, shape, jnp.float32) * deviation * level
    return jnp.minimum(jnp.maximum(drawn, -reach), reach).astype(held_as)


def bell_draw_with(key, extent, deviation, most, shards, heavy, dtype=jnp.bfloat16):
    result = deviation * jax.random.normal(key, extent, jnp.float32)
    if shards:
        result = result * steps_of(key, extent, shards, -0.22, 0.18)
    return jnp.clip(raised(result, jax.random.fold_in(key, 3), *heavy), -most, most).astype(dtype)


def setup_inputs(seed: int = 0) -> dict:
    key_list = jax.random.split(jax.random.key(seed), 16)
    return {
        "resid": centred(key_list[0], (TOKENS, D), 1.0, 6.0, ((0, 64), (1, 8))),
        "norm_gains": jnp.clip(1.0 + 0.18 * jax.random.normal(key_list[1], (3, D), jnp.float32), 0.1, 1.9),
        "gate_one": centred(key_list[2], (D, FF), D ** -0.5, 0.125, ((0, 32), (1, 8))),
        "up_one": centred(key_list[3], (D, FF), D ** -0.5, 0.125, ((0, 32), (1, 8))),
        "down_one": bell_draw_with(key_list[4], (FF, D), FF ** -0.5, 0.15625, ((0, 8), (1, 32)), (0, 1, 32, 2.75)),
        "proj_u": centred(key_list[5], (D, GM), D ** -0.5, 0.125, ((0, 32), (1, 8))),
        "proj_v": centred(key_list[6], (D, GM), D ** -0.5, 0.125, ((0, 32), (1, 8))),
        "spatial": centred(key_list[7], (HEADS, BLOCK, BLOCK), BLOCK ** -0.5, 0.5, ((0, 8),)),
        "spatial_bias": jnp.clip(1.0 + 0.18 * jax.random.normal(key_list[8], (HEADS, BLOCK), jnp.float32), 0.1, 1.9),
        "mix_gain": jnp.clip(1.0 + 0.18 * jax.random.normal(key_list[9], (GM,), jnp.float32), 0.1, 1.9),
        "head_gain": jnp.clip(1.0 + 0.18 * jax.random.normal(key_list[10], (GM,), jnp.float32), 0.1, 1.9),
        "proj_out": bell_draw_with(key_list[11], (GM, D), GM ** -0.5, 0.375, ((0, 8), (1, 32)), (0, 1, 32, 2.75)),
        "gate_two": centred(key_list[12], (D, FF), D ** -0.5, 0.125, ((0, 32), (1, 8))),
        "up_two": centred(key_list[13], (D, FF), D ** -0.5, 0.125, ((0, 32), (1, 8))),
        "down_two": bell_draw_with(key_list[14], (FF, D), FF ** -0.5, 0.15625, ((0, 8), (1, 32)), (0, 1, 32, 2.75)),
    }


def rms_scale(values, gain):
    return values * lax.rsqrt(lax.optimization_barrier(jnp.mean(values * values, axis=-1, keepdims=True)) + 1e-06) * gain

def blockwise_sum(hidden, weight, parts):
    width = hidden.shape[1] // parts
    total = jnp.zeros((hidden.shape[0], weight.shape[1]), jnp.float32)
    for index in range(parts):
        partial_sum = jnp.dot(hidden[:, index * width:(index + 1) * width], weight[index * width:(index + 1) * width], preferred_element_type=jnp.float32)
        rounded = lax.optimization_barrier(partial_sum.astype(jnp.bfloat16))
        total = total + rounded.astype(jnp.float32)
    return total

def feed_forward(stream, gain, gate_weight, up_weight, down_weight):
    normed = rms_scale(stream.astype(jnp.float32), gain).astype(jnp.bfloat16)
    gate = jnp.dot(normed, gate_weight, preferred_element_type=jnp.float32)
    up_part = jnp.dot(normed, up_weight, preferred_element_type=jnp.float32)
    hidden = (jax.nn.silu(gate) * up_part).astype(jnp.bfloat16)
    return blockwise_sum(hidden, down_weight, N_TP)

def reference(resid, norm_gains, gate_one, up_one, down_one, proj_u, proj_v, spatial, spatial_bias, mix_gain, head_gain, proj_out, gate_two, up_two, down_two):
    first = (resid.astype(jnp.float32) + 0.5 * feed_forward(resid, norm_gains[0], gate_one, up_one, down_one)).astype(jnp.bfloat16)
    mnormed = rms_scale(first.astype(jnp.float32), norm_gains[1]).astype(jnp.bfloat16)
    u_part = jnp.dot(mnormed, proj_u, preferred_element_type=jnp.float32)
    v_part = jnp.dot(mnormed, proj_v, preferred_element_type=jnp.float32)
    rows = u_part.shape[0]
    seqs = rows // BLOCK
    gated_u = jax.nn.gelu(u_part).reshape(seqs, BLOCK, HEADS, HEAD_DIM)
    gated_v = jax.nn.gelu(v_part).reshape(seqs, BLOCK, HEADS, HEAD_DIM)
    centre = lax.optimization_barrier(jnp.mean(gated_v, axis=-1, keepdims=True))
    spread = lax.optimization_barrier(jnp.mean(jnp.square(gated_v - centre), axis=-1, keepdims=True))
    vn = ((gated_v - centre) * lax.rsqrt(spread + 1e-05) * mix_gain.reshape(HEADS, HEAD_DIM)).astype(jnp.bfloat16)
    segment = jnp.arange(BLOCK) // SPAN
    causal = segment[:, None] >= segment[None, :]
    masked = jnp.where(causal[None], spatial.astype(jnp.float32), 0.0)
    mixed = jnp.einsum('hts,bshd->bthd', masked, vn.astype(jnp.float32)) + spatial_bias.T[None, :, :, None]
    product = gated_u * mixed
    gated = rms_scale(product, head_gain.reshape(HEADS, HEAD_DIM)).astype(jnp.bfloat16).reshape(rows, HEADS * HEAD_DIM)
    branch = blockwise_sum(gated, proj_out, N_TP)
    second = (first.astype(jnp.float32) + branch).astype(jnp.bfloat16)
    return (second.astype(jnp.float32) + 0.5 * feed_forward(second, norm_gains[2], gate_two, up_two, down_two)).astype(jnp.bfloat16)
```

```python
import functools
import heapq

import jax
import jax.numpy as jnp
from jax import lax
from jax.experimental import pallas as pl
from jax.experimental.pallas import tpu as pltpu
from jax.sharding import PartitionSpec as P

MESH = pl.DeviceIdType.MESH
BF16, F32 = jnp.bfloat16, jnp.float32
SHARD = 64
ITEMS = {
    "a1": (768, 32),
    "b1": (640, 48),
    "d1": (640, 48),
    "m": (512, 32),
    "a2": (768, 32),
    "b2": (640, 48),
    "d2": (640, 32),
}
NAMES = tuple(ITEMS)
RATE = {"y+": 46600.0, "y-": 46600.0, "z+": 46600.0, "z-": 46600.0, "x+": 46600.0, "x-": 46600.0, "d": 250000.0}
DELAY = {"d": 1.5}
AHEAD = 5.0
BLOCK_BYTES = 256 * 256 * 2
Y_FIRST, Z_FIRST = 0, 1
TWICE_UP = (-3, -1, 1, 3)


def rows_of(name, part):
    return ITEMS[name][1] if part == Y_FIRST else SHARD - ITEMS[name][1]


def children(part, dy, dz):
    out = []
    if part == Y_FIRST:
        if dz == 0:
            if 0 <= dy < 4:
                out.append(("y+", dy + 1, 0))
            if -3 < dy <= 0:
                out.append(("y-", dy - 1, 0))
            out += [("z+", dy, 1), ("z-", dy, -1)]
        elif dz == 1 and dy in TWICE_UP:
            out.append(("z+", dy, 2))
        elif dz == -1 and dy not in TWICE_UP:
            out.append(("z-", dy, -2))
    else:
        up, down = (4, 3) if dz == 2 else (3, 4)
        if dy == 0:
            if dz == 0:
                out += [("z+", 0, 1), ("z-", 0, -1)]
            elif dz == 1:
                out.append(("z+", 0, 2))
            out += [("y+", 1, dz), ("y-", -1, dz)]
        elif 0 < dy < up:
            out.append(("y+", dy + 1, dz))
        elif -down < dy < 0:
            out.append(("y-", dy - 1, dz))
    return out


def depth(part, dy, dz):
    return max((1 + depth(part, a, b) for _, a, b in children(part, dy, dz)), default=0)


def gather_steps(stage):
    block, half = BLOCK_BYTES, BLOCK_BYTES // 2
    return {
        "own": [("x+", block, "m1"), ("x-", block, "p1"), ("d", block, "end")],
        "m1": [("x+", half, "h0"), ("d", block, "end")],
        "p1": [("x-", half, "h1"), ("d", block, "end")],
        "h0": [("d", half, "end")],
        "h1": [("d", half, "end")],
    }


def chain():
    half = BLOCK_BYTES // 2
    steps = []
    for s in range(3):
        steps.append((("norm", s), [("ag", s)], 1.5, []))
        if s == 1:
            steps.append((("mix", s), [("w", "m")], 2.5, []))
        else:
            a, b, d = ("a1", "b1", "d1") if s == 0 else ("a2", "b2", "d2")
            for j in range(3):
                steps.append((("gu", s, j), [("w", a), ("w", b)], 1.0, []))
        needs = [("w", "m")] if s == 1 else [("w", d), ("w", "m")]
        for r in (2, 1, 3, 0):
            steps.append((("down", s, r, 1), needs, 0.4, [("d", BLOCK_BYTES, ("rs", s, "pr"), ("pr", s, r))]))
        for r in (2, 1, 3, 0):
            steps.append((("down", s, r, 0), [], 0.4, []))
        steps.append(
            (
                ("pair", s),
                [("rs", s, "pr")],
                0.8,
                [
                    ("x+", half, ("rs", s, "l0"), ("l0", s)),
                    ("x-", half, ("rs", s, "l1"), ("l1", s)),
                    ("x+", half, ("rs", s, "ra"), ("ra1", s)),
                    ("x-", half, ("rs", s, "rb"), ("rb0", s)),
                ],
            )
        )
        steps.append((("relay0", s), [("rs", s, "l0")], 0.2, [("x+", half, ("rs", s, "ra"), ("ra0", s))]))
        steps.append((("relay1", s), [("rs", s, "l1")], 0.2, [("x-", half, ("rs", s, "rb"), ("rb1", s))]))
        steps.append((("end", s), [("rs", s, "ra"), ("rs", s, "rb")], 0.4, [("next", s)]))
    return steps


@functools.lru_cache(None)
def plan():
    count = {}
    for name in NAMES:
        for part in (Y_FIRST, Z_FIRST):
            count[("w", name, part)] = 0

    def nodes(part, dy=0, dz=0):
        yield dy, dz
        for _, a, b in children(part, dy, dz):
            yield from nodes(part, a, b)

    for name in NAMES:
        for part in (Y_FIRST, Z_FIRST):
            count[("w", name, part)] = sum(not children(part, *n) for n in nodes(part))
    expected = {}
    for s in range(3):
        expected[("ag", s)] = 5
        expected[("rs", s, "pr")] = 4
        expected[("rs", s, "l0")] = expected[("rs", s, "l1")] = 1
        expected[("rs", s, "ra")] = expected[("rs", s, "rb")] = 2
    ops, now, serial = [], 0.0, 0
    free = {link: 0.0 for link in RATE}
    ready = {link: [] for link in RATE}
    arrivals, waited = [], set()

    def offer(link, priority, size, landing, op):
        nonlocal serial
        serial += 1
        heapq.heappush(ready[link], (priority, serial, size, landing, op))

    def offer_weight(index, name, part, dy, dz):
        for link, a, b in children(part, dy, dz):
            offer(
                link,
                (index, -depth(part, a, b)),
                rows_of(name, part) * ITEMS[name][0] * 2,
                ("w", index, name, part, a, b),
                ("send", name, part, dy, dz, link, a, b),
            )

    def offer_block(s, at):
        for link, size, landing in gather_steps(s)[at]:
            offer(link, (0, s), size, ("ag", s, landing), ("pass", s, at, link))

    def pump():
        nonlocal serial
        for link, queue in ready.items():
            while queue and free[link] - now < AHEAD:
                _, _, size, landing, op = heapq.heappop(queue)
                free[link] = max(free[link], now) + size / RATE[link]
                serial += 1
                heapq.heappush(arrivals, (free[link] + DELAY.get(link, 2.3), serial, landing))
                ops.append(op)

    for index, name in enumerate(NAMES):
        for part in (Y_FIRST, Z_FIRST):
            offer_weight(index, name, part, 0, 0)
    offer_block(0, "own")
    todo = chain()
    landed_all, times = 0, {}
    while todo or arrivals or any(ready.values()):
        while arrivals and arrivals[0][0] <= now:
            _, _, landing = heapq.heappop(arrivals)
            if landing[0] == "w":
                _, index, name, part, dy, dz = landing
                if children(part, dy, dz):
                    ops.append(("got", name, part, dy, dz))
                    offer_weight(index, name, part, dy, dz)
                else:
                    count[("w", name, part)] -= 1
            elif landing[0] == "ag" and landing[2] != "end":
                ops.append(("block", landing[1], landing[2]))
                offer_block(landing[1], landing[2])
            else:
                key = landing[:2] if landing[0] == "ag" else landing
                expected[key] -= 1
            times[landing[:3]] = now
        pump()
        if todo:
            step, needs, duration, sends = todo[0]
            done = True
            for need in needs:
                if need[0] == "w":
                    done &= count[("w", need[1], 0)] == 0 and count[("w", need[1], 1)] == 0
                else:
                    done &= expected[need] == 0
            if done:
                for need in needs:
                    if need not in waited:
                        waited.add(need)
                        ops.append(("all",) + need)
                ops.append(("do",) + step)
                times[step] = now
                now += duration
                todo.pop(0)
                for send in sends:
                    if send[0] == "next":
                        if send[1] < 2:
                            offer_block(send[1] + 1, "own")
                    else:
                        offer(send[0], (-1, 0), send[1], send[2], ("rsend",) + send[3])
                continue
        later = [arrivals[0][0]] if arrivals else []
        later += [free[link] - AHEAD + 0.01 for link, queue in ready.items() if queue]
        if not later:
            break
        now = max(min(later), now + 0.01)
    return ops, times, now


def semaphores():
    index, keys = {}, []
    for name in NAMES:
        for part in (Y_FIRST, Z_FIRST):
            index[("all", name, part)] = len(index)
            index[("sent", name, part)] = len(index)
    ops = plan()[0]
    for op in ops:
        if op[0] == "got":
            index[op[1:]] = len(index)
        elif op[0] == "block":
            index[op] = len(index)
        elif op[0] in ("pass", "rsend"):
            index[op] = len(index)
    for s in range(3):
        index[("ag", s)] = len(index)
        for what in ("pr", "l0", "l1", "ra", "rb"):
            index[("rs", s, what)] = len(index)
    return index


def rms_scale(values, mean_square, gain):
    return values * lax.rsqrt(mean_square + 1e-06) * gain


def contract(left, right):
    return lax.dot_general(left, right, (((1,), (1,)), ((), ())), preferred_element_type=F32)


def kernel(sems_of, *refs):
    weights_in = dict(zip(NAMES, refs[:7]))
    resid, gains, spatial, bias, mix_gain, head_gain, out = refs[7:14]
    g = dict(zip(NAMES, refs[14:21]))
    (xg, normed, hidden, ps, pr, po, sb, rl, ra, rb, tt, local_sem, sems) = refs[21:]

    rep, fs, tp = lax.axis_index("rep"), lax.axis_index("fs"), lax.axis_index("tp")
    x, core = tp // 2, tp % 2
    y, z = fs % 8, rep * 4 + fs // 8

    def device(link):
        if link[0] == "y":
            ny = (y + (1 if link[1] == "+" else 7)) % 8
            return {"rep": rep, "fs": (fs // 8) * 8 + ny, "tp": tp}
        if link[0] == "z":
            nz = (z + (1 if link[1] == "+" else 7)) % 8
            return {"rep": nz // 4, "fs": (nz % 4) * 8 + y, "tp": tp}
        if link[0] == "x":
            nx = (x + (1 if link[1] == "+" else 3)) % 4
            return {"rep": rep, "fs": fs, "tp": nx * 2 + core}
        return {"rep": rep, "fs": fs, "tp": x * 2 + 1 - core}

    devices = {link: device(link) for link in RATE}
    barrier = pltpu.get_barrier_semaphore()
    for link in RATE:
        pl.semaphore_signal(barrier, inc=1, device_id=devices[link], device_id_type=MESH)

    own = pl.multiple_of(fs * SHARD, SHARD)
    copies = [
        pltpu.make_async_copy(weights_in[name], g[name].at[pl.ds(own, SHARD)], local_sem.at[k])
        for k, name in enumerate(NAMES)
    ]
    copies.append(pltpu.make_async_copy(resid, xg.at[0, tp], local_sem.at[7]))
    for copy in copies:
        copy.start()
    pl.semaphore_wait(barrier, len(RATE))
    for copy in copies:
        copy.wait()

    def piece(name, part, dy, dz):
        f = ((z + 8 - dz) % 4) * 8 + (y + 8 - dy) % 8
        start = f * SHARD + (0 if part == Y_FIRST else ITEMS[name][1])
        return g[name].at[pl.ds(pl.multiple_of(start, 16), rows_of(name, part))]

    def remote(src, dst, send, recv, link):
        return pltpu.make_async_remote_copy(
            src_ref=src,
            dst_ref=dst,
            send_sem=sems.at[sems_of[send]],
            recv_sem=sems.at[sems_of[recv]],
            device_id=devices[link],
            device_id_type=MESH,
        )

    def wait_for(ref, key):
        pltpu.make_async_copy(ref, ref, sems.at[sems_of[key]]).wait()

    def block_at(s, at):
        shift = {"own": 0, "m1": 3, "p1": 1, "h0": 2, "h1": 2}[at]
        ref = xg.at[s, ((x + shift) % 4) * 2 + core]
        if at[0] == "h":
            return ref.at[pl.ds(0 if at == "h0" else 128, 128)]
        return ref

    def down(s, r, other):
        t = ((x + r) % 4) * 2 + (1 - core if other else core)
        at = pl.ds(pl.multiple_of(t * 256, 256), 256)
        if s == 1:
            total = contract(hidden[:, :128], g["m"][at, 256:384])
        else:
            total = contract(hidden[:, :640], g["d1" if s == 0 else "d2"][at, :])
            total = total + contract(hidden[:, 640:768], g["m"][at, 384:512])
        if other:
            ps[s, r] = total.astype(BF16)
        else:
            po[r] = total

    def gate_up(s, j):
        a, b = (g["a1"], g["b1"]) if s == 0 else (g["a2"], g["b2"])
        first = jnp.dot(normed[...], a[:, 256 * j : 256 * (j + 1)], preferred_element_type=F32)
        if j < 2:
            second = jnp.dot(normed[...], b[:, 256 * j : 256 * (j + 1)], preferred_element_type=F32)
            hidden[:, 256 * j : 256 * (j + 1)] = (jax.nn.silu(first) * second).astype(BF16)
            return
        second = jnp.dot(normed[...], b[:, 512:640], preferred_element_type=F32)
        hidden[:, 512:640] = (jax.nn.silu(first[:, :128]) * second).astype(BF16)
        rest = first[:, 128:]
        value = jax.nn.silu(rest) * pltpu.roll(rest, 64, 1)
        lane = lax.broadcasted_iota(jnp.int32, (256, 128), 1)
        keep = lane < 64 if s == 0 else lane >= 64
        hidden[:, 640:768] = jnp.where(keep, value, 0.0).astype(BF16)

    def norm(s):
        total = jnp.zeros((256, 1), F32)
        for t in range(8):
            values = xg[s, t].astype(F32)
            total = total + jnp.sum(values * values, axis=-1, keepdims=True)
        for t in range(8):
            cols = slice(256 * t, 256 * (t + 1))
            normed[:, cols] = rms_scale(xg[s, t].astype(F32), total / 2048.0, gains[s : s + 1, cols]).astype(BF16)

    def mix():
        both = jnp.dot(normed[...], g["m"][:, 0:256], preferred_element_type=F32)
        u, v = jax.nn.gelu(both[:, :128]), jax.nn.gelu(both[:, 128:])
        centre = jnp.mean(v, axis=-1, keepdims=True)
        spread = jnp.mean(jnp.square(v - centre), axis=-1, keepdims=True)
        vn = ((v - centre) * lax.rsqrt(spread + 1e-05) * mix_gain[...]).astype(BF16)
        to = lax.broadcasted_iota(jnp.int32, (128, 128), 0) // 64
        source = lax.broadcasted_iota(jnp.int32, (128, 128), 1) // 64
        masked = jnp.where(to >= source, spatial[...].astype(F32), 0.0).astype(BF16)
        for k in range(2):
            rows = slice(128 * k, 128 * (k + 1))
            mixed = jnp.dot(masked, vn[rows], preferred_element_type=F32) + bias[...]
            product = u[rows] * mixed
            square = jnp.mean(product * product, axis=-1, keepdims=True)
            hidden[rows, :128] = rms_scale(product, square, head_gain[...]).astype(BF16)

    lower, upper = pl.ds(0, 128), pl.ds(128, 128)
    for op in plan()[0]:
        kind = op[0]
        if kind == "send":
            _, name, part, dy, dz, link, a, b = op
            ref = piece(name, part, dy, dz)
            landing = (name, part, a, b) if children(part, a, b) else ("all", name, part)
            remote(ref, ref, ("sent", name, part), landing, link).start()
        elif kind == "got":
            _, name, part, dy, dz = op
            wait_for(piece(name, part, dy, dz), op[1:])
        elif kind == "pass":
            _, s, at, link = op
            ref = block_at(s, at)
            if link == "d":
                landing = ("ag", s)
            else:
                landing = ("block", s, {"own": {"x+": "m1", "x-": "p1"}, "m1": {"x+": "h0"}, "p1": {"x-": "h1"}}[at][link])
                if at == "m1":
                    ref = ref.at[lower]
                elif at == "p1":
                    ref = ref.at[upper]
            remote(ref, ref, op, landing, link).start()
        elif kind == "block":
            wait_for(block_at(op[1], op[2]), op)
        elif kind == "rsend":
            what, s = op[1], op[2]
            if what == "pr":
                remote(ps.at[s, op[3]], pr.at[s, op[3]], op, ("rs", s, "pr"), "d").start()
            elif what == "l0":
                remote(sb.at[s, 1, lower], rl.at[s, 0], op, ("rs", s, "l0"), "x+").start()
            elif what == "l1":
                remote(sb.at[s, 1, upper], rl.at[s, 1], op, ("rs", s, "l1"), "x-").start()
            elif what == "ra1":
                remote(sb.at[s, 0, upper], ra.at[s, upper], op, ("rs", s, "ra"), "x+").start()
            elif what == "rb0":
                remote(sb.at[s, 2, lower], rb.at[s, lower], op, ("rs", s, "rb"), "x-").start()
            elif what == "ra0":
                remote(tt.at[s, 0], ra.at[s, lower], op, ("rs", s, "ra"), "x+").start()
            elif what == "rb1":
                remote(tt.at[s, 1], rb.at[s, upper], op, ("rs", s, "rb"), "x-").start()
        elif kind == "all":
            if op[1] == "w":
                name = op[2]
                for part, many in ((Y_FIRST, 16), (Z_FIRST, 8)):
                    wait_for(g[name].at[pl.ds(0, many * rows_of(name, part))], ("all", name, part))
            elif op[1] == "ag":
                wait_for(xg.at[op[2], pl.ds(0, 4)], op[1:])
            else:
                _, _, s, what = op
                wait_for({"pr": pr.at[s], "l0": rl.at[s, 0], "l1": rl.at[s, 1], "ra": ra.at[s], "rb": rb.at[s]}[what], op[1:])
        else:
            what, s = op[1], op[2]
            if what == "norm":
                norm(s)
            elif what == "gu":
                gate_up(s, op[3])
            elif what == "mix":
                mix()
            elif what == "down":
                down(s, op[3], op[4])
            elif what == "pair":
                po[0] = po[0] + pr[s, 0].astype(F32)
                for r in (2, 1, 3):
                    sb[s, r - 1] = (po[r] + pr[s, r].astype(F32)).astype(BF16)
            elif what == "relay0":
                tt[s, 0] = (sb[s, 0, :128].astype(F32) + rl[s, 0].astype(F32)).astype(BF16)
            elif what == "relay1":
                tt[s, 1] = (sb[s, 2, 128:].astype(F32) + rl[s, 1].astype(F32)).astype(BF16)
            else:
                total = po[0] + ra[s].astype(F32) + rb[s].astype(F32)
                value = (xg[s, tp].astype(F32) + (1.0 if s == 1 else 0.5) * total).astype(BF16)
                if s < 2:
                    xg[s + 1, tp] = value
                else:
                    out[...] = value

    for name in NAMES:
        for part in (Y_FIRST, Z_FIRST):
            wait_for(g[name].at[pl.ds(0, 31 * rows_of(name, part))], ("sent", name, part))
    for op in plan()[0]:
        if op[0] == "pass":
            ref = block_at(op[1], op[2])
            if op[2] in ("m1", "p1") and op[3] != "d":
                ref = ref.at[lower]
            wait_for(ref, op)
        elif op[0] == "rsend":
            wait_for(ps.at[op[2], 0] if op[1] == "pr" else rl.at[op[2], 0], op)


def body(resid, norm_gains, gate_one, up_one, down_one, proj_u, proj_v, spatial, spatial_bias, mix_gain, head_gain, proj_out, gate_two, up_two, down_two):
    turned_one, turned_two = down_one.T, down_two.T
    weights = {
        "a1": jnp.concatenate([gate_one, up_one[:, 640:]], axis=1),
        "b1": up_one[:, :640],
        "d1": turned_one[:, :640],
        "m": jnp.concatenate([proj_u, proj_v, proj_out.T, turned_one[:, 640:], turned_two[:, 640:]], axis=1),
        "a2": jnp.concatenate([gate_two[:, :640], up_two[:, 640:], gate_two[:, 640:]], axis=1),
        "b2": up_two[:, :640],
        "d2": turned_two[:, :640],
    }
    sems_of = semaphores()
    rows, width = resid.shape
    anywhere = pl.BlockSpec(memory_space=pltpu.HBM)
    vmem = pl.BlockSpec(memory_space=pltpu.VMEM)
    return pl.pallas_call(
        functools.partial(kernel, sems_of),
        out_shape=jax.ShapeDtypeStruct((rows, width), BF16),
        in_specs=[anywhere] * 8 + [vmem] * 5,
        out_specs=vmem,
        scratch_shapes=[pltpu.VMEM((2048, ITEMS[name][0]), BF16) for name in NAMES]
        + [
            pltpu.VMEM((3, 8, 256, 256), BF16),
            pltpu.VMEM((256, 2048), BF16),
            pltpu.VMEM((256, 768), BF16),
            pltpu.VMEM((3, 4, 256, 256), BF16),
            pltpu.VMEM((3, 4, 256, 256), BF16),
            pltpu.VMEM((4, 256, 256), F32),
            pltpu.VMEM((3, 3, 256, 256), BF16),
            pltpu.VMEM((3, 2, 128, 256), BF16),
            pltpu.VMEM((3, 256, 256), BF16),
            pltpu.VMEM((3, 256, 256), BF16),
            pltpu.VMEM((3, 2, 128, 256), BF16),
            pltpu.SemaphoreType.DMA((8,)),
            pltpu.SemaphoreType.DMA((len(sems_of),)),
        ],
        compiler_params=pltpu.CompilerParams(collective_id=0, has_side_effects=True, vmem_limit_bytes=60 * 2**20),
        name="layer",
    )(
        *[weights[name] for name in NAMES],
        resid,
        norm_gains,
        spatial[0],
        spatial_bias.reshape(128, 1),
        mix_gain.reshape(1, 128),
        head_gain.reshape(1, 128),
    )


def solution(mesh):
    in_specs = (
        P(("rep", "fs"), "tp"),
        P(),
        P("fs", "tp"),
        P("fs", "tp"),
        P("tp", "fs"),
        P("fs", "tp"),
        P("fs", "tp"),
        P("tp", None, None),
        P("tp", None),
        P("tp"),
        P("tp"),
        P("tp", "fs"),
        P("fs", "tp"),
        P("fs", "tp"),
        P("tp", "fs"),
    )
    return jax.shard_map(body, mesh=mesh, in_specs=in_specs, out_specs=P(("rep", "fs"), "tp"), check_vma=False)
```

```python
import functools
import heapq

import jax
import jax.numpy as jnp
from jax import lax
from jax.experimental import pallas as pl
from jax.experimental.pallas import tpu as pltpu
from jax.sharding import PartitionSpec as P

MESH = pl.DeviceIdType.MESH
BF16, F32 = jnp.bfloat16, jnp.float32
SHARD = 64
ITEMS = {
    "a1": (768, 32),
    "b1": (640, 48),
    "d1": (768, 32),
    "m": (384, 48),
    "a2": (768, 32),
    "b2": (640, 48),
    "d2": (640, 32),
}
NAMES = tuple(ITEMS)
RATE = {"y+": 46600.0, "y-": 46600.0, "z+": 46600.0, "z-": 46600.0, "x+": 46600.0, "x-": 46600.0, "d": 250000.0}
DELAY = {"d": 1.5}
AHEAD = 2.0
ROWS = 128
HALF = 64
BLOCK_BYTES = ROWS * 256 * 2
STREAMS = 2
Y_FIRST, Z_FIRST = 0, 1
TWICE_UP = (-3, -1, 1, 3)


def rows_of(name, part):
    return ITEMS[name][1] if part == Y_FIRST else SHARD - ITEMS[name][1]


def children(part, dy, dz):
    out = []
    if part == Y_FIRST:
        if dz == 0:
            if 0 <= dy < 4:
                out.append(("y+", dy + 1, 0))
            if -3 < dy <= 0:
                out.append(("y-", dy - 1, 0))
            out += [("z+", dy, 1), ("z-", dy, -1)]
        elif dz == 1 and dy in TWICE_UP:
            out.append(("z+", dy, 2))
        elif dz == -1 and dy not in TWICE_UP:
            out.append(("z-", dy, -2))
    else:
        up, down = (4, 3) if dz == 2 else (3, 4)
        if dy == 0:
            if dz == 0:
                out += [("z+", 0, 1), ("z-", 0, -1)]
            elif dz == 1:
                out.append(("z+", 0, 2))
            out += [("y+", 1, dz), ("y-", -1, dz)]
        elif 0 < dy < up:
            out.append(("y+", dy + 1, dz))
        elif -down < dy < 0:
            out.append(("y-", dy - 1, dz))
    return out


def depth(part, dy, dz):
    return max((1 + depth(part, a, b) for _, a, b in children(part, dy, dz)), default=0)


def gather_steps():
    block, half = BLOCK_BYTES, BLOCK_BYTES // 2
    return {
        "own": [("x+", block, "m1"), ("x-", block, "p1"), ("d", block, "end")],
        "m1": [("x+", half, "h0"), ("d", block, "end")],
        "p1": [("x-", half, "h1"), ("d", block, "end")],
        "h0": [("d", half, "end")],
        "h1": [("d", half, "end")],
    }


def chain(h):
    half = BLOCK_BYTES // 2
    steps = []
    for s in range(3):
        steps.append((("norm", s, h), [("ag", s, h)], 0.8, []))
        if s == 1:
            steps.append((("mix", s, h), [("w", "m")], 1.3, []))
        else:
            a, b, d = ("a1", "b1", "d1") if s == 0 else ("a2", "b2", "d2")
            for j in range(3):
                steps.append((("gu", s, h, j), [("w", a), ("w", b)], 0.6, []))
        needs = [("w", "m")] if s == 1 else [("w", "d1"), ("w", d)]
        for r in (2, 1, 3, 0):
            steps.append((("down", s, h, r, 1), needs, 0.25, [("d", BLOCK_BYTES, ("rs", s, h, "pr"), ("pr", s, h, r))]))
        for r in (2, 1, 3, 0):
            steps.append((("down", s, h, r, 0), [], 0.25, []))
        key = ("rs", s, h)
        steps.append(
            (
                ("pair", s, h),
                [key + ("pr",)],
                0.5,
                [
                    ("x+", half, key + ("l0",), ("l0", s, h)),
                    ("x-", half, key + ("l1",), ("l1", s, h)),
                    ("x+", half, key + ("ra",), ("ra1", s, h)),
                    ("x-", half, key + ("rb",), ("rb0", s, h)),
                ],
            )
        )
        steps.append((("relay0", s, h), [key + ("l0",)], 0.15, [("x+", half, key + ("ra",), ("ra0", s, h))]))
        steps.append((("relay1", s, h), [key + ("l1",)], 0.15, [("x-", half, key + ("rb",), ("rb1", s, h))]))
        steps.append((("end", s, h), [key + ("ra",), key + ("rb",)], 0.3, [("next", s)]))
    return steps


@functools.lru_cache(None)
def plan():
    count = {}
    for name in NAMES:
        for part in (Y_FIRST, Z_FIRST):
            count[("w", name, part)] = 0

    def nodes(part, dy=0, dz=0):
        yield dy, dz
        for _, a, b in children(part, dy, dz):
            yield from nodes(part, a, b)

    for name in NAMES:
        for part in (Y_FIRST, Z_FIRST):
            count[("w", name, part)] = sum(not children(part, *n) for n in nodes(part))
    expected = {}
    for s in range(3):
        for h in range(STREAMS):
            expected[("ag", s, h)] = 5
            expected[("rs", s, h, "pr")] = 4
            expected[("rs", s, h, "l0")] = expected[("rs", s, h, "l1")] = 1
            expected[("rs", s, h, "ra")] = expected[("rs", s, h, "rb")] = 2
    ops, now, serial = [], 0.0, 0
    free = {link: 0.0 for link in RATE}
    ready = {link: [] for link in RATE}
    arrivals, waited = [], set()

    def offer(link, priority, size, landing, op):
        nonlocal serial
        serial += 1
        heapq.heappush(ready[link], (priority, serial, size, landing, op))

    def offer_weight(index, name, part, dy, dz):
        for link, a, b in children(part, dy, dz):
            offer(
                link,
                (index, -depth(part, a, b)),
                rows_of(name, part) * ITEMS[name][0] * 2,
                ("w", index, name, part, a, b),
                ("send", name, part, dy, dz, link, a, b),
            )

    def offer_block(s, h, at):
        for link, size, landing in gather_steps()[at]:
            offer(link, (h, s), size, ("ag", s, h, landing), ("pass", s, h, at, link))

    def pump():
        nonlocal serial
        for link, queue in ready.items():
            while queue and free[link] - now < AHEAD:
                _, _, size, landing, op = heapq.heappop(queue)
                free[link] = max(free[link], now) + size / RATE[link]
                serial += 1
                heapq.heappush(arrivals, (free[link] + DELAY.get(link, 2.3), serial, landing))
                ops.append(op)

    for index, name in enumerate(NAMES):
        for part in (Y_FIRST, Z_FIRST):
            offer_weight(index, name, part, 0, 0)
    for h in range(STREAMS):
        offer_block(0, h, "own")
    chains = [chain(h) for h in range(STREAMS)]
    times = {}
    while any(chains) or arrivals or any(ready.values()):
        while arrivals and arrivals[0][0] <= now:
            _, _, landing = heapq.heappop(arrivals)
            if landing[0] == "w":
                _, index, name, part, dy, dz = landing
                if children(part, dy, dz):
                    ops.append(("got", name, part, dy, dz))
                    offer_weight(index, name, part, dy, dz)
                else:
                    count[("w", name, part)] -= 1
            elif landing[0] == "ag" and landing[3] != "end":
                ops.append(("block",) + landing[1:])
                offer_block(*landing[1:])
            else:
                key = landing[:3] if landing[0] == "ag" else landing
                expected[key] -= 1
            times[landing[:3]] = now
        pump()
        ran = False
        for h, todo in enumerate(chains):
            if not todo:
                continue
            step, needs, duration, sends = todo[0]
            done = True
            for need in needs:
                if need[0] == "w":
                    done &= count[("w", need[1], 0)] == 0 and count[("w", need[1], 1)] == 0
                else:
                    done &= expected[need] == 0
            if not done:
                continue
            for need in needs:
                if need not in waited:
                    waited.add(need)
                    ops.append(("all",) + need)
            ops.append(("do",) + step)
            times[step] = now
            now += duration
            todo.pop(0)
            for send in sends:
                if send[0] == "next":
                    if send[1] < 2:
                        offer_block(send[1] + 1, h, "own")
                else:
                    offer(send[0], (-1, 0), send[1], send[2], ("rsend",) + send[3])
            ran = True
            break
        if ran:
            continue
        later = [arrivals[0][0]] if arrivals else []
        later += [free[link] - AHEAD + 0.01 for link, queue in ready.items() if queue]
        if not later:
            break
        now = max(min(later), now + 0.01)
    return ops, times, now


def semaphores():
    index, keys = {}, []
    for name in NAMES:
        for part in (Y_FIRST, Z_FIRST):
            index[("all", name, part)] = len(index)
            index[("sent", name, part)] = len(index)
    ops = plan()[0]
    for op in ops:
        if op[0] == "got":
            index[op[1:]] = len(index)
        elif op[0] == "block":
            index[op] = len(index)
        elif op[0] in ("pass", "rsend"):
            index[op] = len(index)
    for s in range(3):
        for h in range(STREAMS):
            index[("ag", s, h)] = len(index)
            for what in ("pr", "l0", "l1", "ra", "rb"):
                index[("rs", s, h, what)] = len(index)
    return index


def rms_scale(values, mean_square, gain):
    return values * lax.rsqrt(mean_square + 1e-06) * gain


def contract(left, right):
    return lax.dot_general(left, right, (((1,), (1,)), ((), ())), preferred_element_type=F32)


def kernel(sems_of, *refs):
    gate_one, up_one, down_one, proj_u, proj_v, proj_out, gate_two, up_two, down_two = refs[:9]
    resid, small_in, out = refs[9], refs[10:15], refs[15]
    g = dict(zip(NAMES, refs[16:23]))
    (xg, normed, hidden, ps, pr, po, sb, rl, ra, rb, tt) = refs[23:34]
    raw, small, local_sem, sems = refs[34:41], refs[41:46], refs[46], refs[47]
    gains, spatial, bias, mix_gain, head_gain = small

    rep, fs, tp = lax.axis_index("rep"), lax.axis_index("fs"), lax.axis_index("tp")
    x, core = tp // 2, tp % 2
    y, z = fs % 8, rep * 4 + fs // 8

    def device(link):
        if link[0] == "y":
            ny = (y + (1 if link[1] == "+" else 7)) % 8
            return {"rep": rep, "fs": (fs // 8) * 8 + ny, "tp": tp}
        if link[0] == "z":
            nz = (z + (1 if link[1] == "+" else 7)) % 8
            return {"rep": nz // 4, "fs": (nz % 4) * 8 + y, "tp": tp}
        if link[0] == "x":
            nx = (x + (1 if link[1] == "+" else 3)) % 4
            return {"rep": rep, "fs": fs, "tp": nx * 2 + core}
        return {"rep": rep, "fs": fs, "tp": x * 2 + 1 - core}

    devices = {link: device(link) for link in RATE}
    barrier = pltpu.get_barrier_semaphore()
    for link in RATE:
        pl.semaphore_signal(barrier, inc=1, device_id=devices[link], device_id_type=MESH)

    own = pl.multiple_of(fs * SHARD, SHARD)
    rows = pl.ds(own, SHARD)
    pairs = [
        (up_one.at[:, pl.ds(0, 640)], g["b1"].at[rows]),
        (gate_one.at[:, pl.ds(0, 640)], g["a1"].at[rows, pl.ds(0, 640)]),
        (up_two.at[:, pl.ds(0, 640)], g["b2"].at[rows]),
        (gate_two.at[:, pl.ds(0, 640)], g["a2"].at[rows, pl.ds(0, 640)]),
        (proj_u, g["m"].at[rows, pl.ds(0, 128)]),
        (proj_v, g["m"].at[rows, pl.ds(128, 128)]),
        (resid, xg.at[0, tp]),
    ]
    first_copies = len(pairs)
    pairs += list(zip((gate_one, up_one, gate_two, up_two, down_one, down_two, proj_out), raw))
    pairs += list(zip(small_in, small))
    copies = [pltpu.make_async_copy(src, dst, local_sem.at[k]) for k, (src, dst) in enumerate(pairs)]
    for copy in copies[first_copies:] + copies[:first_copies]:
        copy.start()
    for copy in copies[first_copies:]:
        copy.wait()
    one = jnp.where(
        lax.broadcasted_iota(jnp.int32, (SHARD, SHARD), 0) == lax.broadcasted_iota(jnp.int32, (SHARD, SHARD), 1), 1.0, 0.0
    ).astype(BF16)

    def turned(ref):
        return contract(one, ref[...]).astype(BF16)

    g["a1"][rows, 640:768] = jnp.concatenate([raw[0][:, 640:704], raw[1][:, 640:704]], axis=1)
    g["a2"][rows, 640:768] = jnp.concatenate([raw[3][:, 640:704], raw[2][:, 640:704]], axis=1)
    down_a, down_b = turned(raw[4]), turned(raw[5])
    g["d1"][rows, 0:640] = down_a[:, :640]
    g["d1"][rows, 640:768] = jnp.concatenate([down_a[:, 640:704], down_b[:, 640:704]], axis=1)
    g["d2"][rows, :] = down_b[:, :640]
    g["m"][rows, 256:384] = turned(raw[6])
    pl.semaphore_wait(barrier, len(RATE))
    for copy in copies[:first_copies]:
        copy.wait()

    def piece(name, part, dy, dz):
        f = ((z + 8 - dz) % 4) * 8 + (y + 8 - dy) % 8
        start = f * SHARD + (0 if part == Y_FIRST else ITEMS[name][1])
        return g[name].at[pl.ds(pl.multiple_of(start, 16), rows_of(name, part))]

    def remote(src, dst, send, recv, link):
        return pltpu.make_async_remote_copy(
            src_ref=src,
            dst_ref=dst,
            send_sem=sems.at[sems_of[send]],
            recv_sem=sems.at[sems_of[recv]],
            device_id=devices[link],
            device_id_type=MESH,
        )

    def wait_for(ref, key):
        pltpu.make_async_copy(ref, ref, sems.at[sems_of[key]]).wait()

    def block_at(s, h, at):
        shift = {"own": 0, "m1": 3, "p1": 1, "h0": 2, "h1": 2}[at]
        start, size = h * ROWS, ROWS
        if at[0] == "h":
            start, size = start + (0 if at == "h0" else HALF), HALF
        return xg.at[s, ((x + shift) % 4) * 2 + core, pl.ds(start, size)]

    def down(s, h, r, other):
        t = ((x + r) % 4) * 2 + (1 - core if other else core)
        at = pl.ds(pl.multiple_of(t * 256, 256), 256)
        if s == 1:
            total = contract(hidden[h, :, :128], g["m"][at, 256:384])
        elif s == 0:
            total = contract(hidden[h], g["d1"][at, :])
        else:
            total = contract(hidden[h, :, :640], g["d2"][at, :])
            total = total + contract(hidden[h, :, 640:768], g["d1"][at, 640:768])
        if other:
            ps[s, h, r] = total.astype(BF16)
        else:
            po[h, r] = total

    def gate_up(s, h, j):
        a, b = (g["a1"], g["b1"]) if s == 0 else (g["a2"], g["b2"])
        first = jnp.dot(normed[h], a[:, 256 * j : 256 * (j + 1)], preferred_element_type=F32)
        if j < 2:
            second = jnp.dot(normed[h], b[:, 256 * j : 256 * (j + 1)], preferred_element_type=F32)
            hidden[h, :, 256 * j : 256 * (j + 1)] = (jax.nn.silu(first) * second).astype(BF16)
            return
        second = jnp.dot(normed[h], b[:, 512:640], preferred_element_type=F32)
        hidden[h, :, 512:640] = (jax.nn.silu(first[:, :128]) * second).astype(BF16)
        rest = first[:, 128:]
        value = jax.nn.silu(rest) * pltpu.roll(rest, 64, 1)
        lane = lax.broadcasted_iota(jnp.int32, (ROWS, 128), 1)
        keep = lane < 64 if s == 0 else lane >= 64
        hidden[h, :, 640:768] = jnp.where(keep, value, 0.0).astype(BF16)

    def norm(s, h):
        rows = slice(h * ROWS, (h + 1) * ROWS)
        total = jnp.zeros((ROWS, 1), F32)
        for t in range(8):
            values = xg[s, t, rows].astype(F32)
            total = total + jnp.sum(values * values, axis=-1, keepdims=True)
        for t in range(8):
            cols = slice(256 * t, 256 * (t + 1))
            scaled = rms_scale(xg[s, t, rows].astype(F32), total / 2048.0, gains[s : s + 1, cols])
            normed[h, :, cols] = scaled.astype(BF16)

    def mix(h):
        both = jnp.dot(normed[h], g["m"][:, 0:256], preferred_element_type=F32)
        u, v = jax.nn.gelu(both[:, :128]), jax.nn.gelu(both[:, 128:])
        centre = jnp.mean(v, axis=-1, keepdims=True)
        spread = jnp.mean(jnp.square(v - centre), axis=-1, keepdims=True)
        vn = ((v - centre) * lax.rsqrt(spread + 1e-05) * mix_gain[...]).astype(BF16)
        to, source = lax.broadcasted_iota(jnp.int32, (128, 128), 0), lax.broadcasted_iota(jnp.int32, (128, 128), 1)
        masked = jnp.where(to // 64 >= source // 64, spatial[0].astype(F32), 0.0).astype(BF16)
        offset = jnp.sum(jnp.where(to == source, bias[...], 0.0), axis=-1, keepdims=True)
        product = u * (jnp.dot(masked, vn, preferred_element_type=F32) + offset)
        square = jnp.mean(product * product, axis=-1, keepdims=True)
        hidden[h, :, :128] = rms_scale(product, square, head_gain[...]).astype(BF16)

    lower, upper = pl.ds(0, HALF), pl.ds(HALF, HALF)
    for op in plan()[0]:
        kind = op[0]
        if kind == "send":
            _, name, part, dy, dz, link, a, b = op
            ref = piece(name, part, dy, dz)
            landing = (name, part, a, b) if children(part, a, b) else ("all", name, part)
            remote(ref, ref, ("sent", name, part), landing, link).start()
        elif kind == "got":
            _, name, part, dy, dz = op
            wait_for(piece(name, part, dy, dz), op[1:])
        elif kind == "pass":
            _, s, h, at, link = op
            ref = block_at(s, h, at)
            if link == "d":
                landing = ("ag", s, h)
            else:
                arrived = {"own": {"x+": "m1", "x-": "p1"}, "m1": {"x+": "h0"}, "p1": {"x-": "h1"}}[at][link]
                landing = ("block", s, h, arrived)
                if at == "m1":
                    ref = ref.at[lower]
                elif at == "p1":
                    ref = ref.at[upper]
            remote(ref, ref, op, landing, link).start()
        elif kind == "block":
            wait_for(block_at(*op[1:]), op)
        elif kind == "rsend":
            what, s, h = op[1:4]
            key = ("rs", s, h)
            if what == "pr":
                remote(ps.at[s, h, op[4]], pr.at[s, h, op[4]], op, key + ("pr",), "d").start()
            elif what == "l0":
                remote(sb.at[s, h, 1, lower], rl.at[s, h, 0], op, key + ("l0",), "x+").start()
            elif what == "l1":
                remote(sb.at[s, h, 1, upper], rl.at[s, h, 1], op, key + ("l1",), "x-").start()
            elif what == "ra1":
                remote(sb.at[s, h, 0, upper], ra.at[s, h, upper], op, key + ("ra",), "x+").start()
            elif what == "rb0":
                remote(sb.at[s, h, 2, lower], rb.at[s, h, lower], op, key + ("rb",), "x-").start()
            elif what == "ra0":
                remote(tt.at[s, h, 0], ra.at[s, h, lower], op, key + ("ra",), "x+").start()
            elif what == "rb1":
                remote(tt.at[s, h, 1], rb.at[s, h, upper], op, key + ("rb",), "x-").start()
        elif kind == "all":
            if op[1] == "w":
                name = op[2]
                for part, many in ((Y_FIRST, 16), (Z_FIRST, 8)):
                    wait_for(g[name].at[pl.ds(0, many * rows_of(name, part))], ("all", name, part))
            elif op[1] == "ag":
                wait_for(xg.at[op[2], pl.ds(0, 4), pl.ds(op[3] * ROWS, ROWS)], op[1:])
            else:
                _, _, s, h, what = op
                at = {"pr": pr.at[s, h], "l0": rl.at[s, h, 0], "l1": rl.at[s, h, 1], "ra": ra.at[s, h], "rb": rb.at[s, h]}
                wait_for(at[what], op[1:])
        else:
            what, s, h = op[1:4]
            if what == "norm":
                norm(s, h)
            elif what == "gu":
                gate_up(s, h, op[4])
            elif what == "mix":
                mix(h)
            elif what == "down":
                down(s, h, op[4], op[5])
            elif what == "pair":
                po[h, 0] = po[h, 0] + pr[s, h, 0].astype(F32)
                for r in (2, 1, 3):
                    sb[s, h, r - 1] = (po[h, r] + pr[s, h, r].astype(F32)).astype(BF16)
            elif what == "relay0":
                tt[s, h, 0] = (sb[s, h, 0, :HALF].astype(F32) + rl[s, h, 0].astype(F32)).astype(BF16)
            elif what == "relay1":
                tt[s, h, 1] = (sb[s, h, 2, HALF:].astype(F32) + rl[s, h, 1].astype(F32)).astype(BF16)
            else:
                at = slice(h * ROWS, (h + 1) * ROWS)
                total = po[h, 0] + ra[s, h].astype(F32) + rb[s, h].astype(F32)
                value = (xg[s, tp, at].astype(F32) + (1.0 if s == 1 else 0.5) * total).astype(BF16)
                if s < 2:
                    xg[s + 1, tp, at] = value
                else:
                    out[at, :] = value

    for name in NAMES:
        for part in (Y_FIRST, Z_FIRST):
            wait_for(g[name].at[pl.ds(0, 31 * rows_of(name, part))], ("sent", name, part))
    for op in plan()[0]:
        if op[0] == "pass":
            ref = block_at(op[1], op[2], op[3])
            if op[3] in ("m1", "p1") and op[4] != "d":
                ref = ref.at[lower]
            wait_for(ref, op)
        elif op[0] == "rsend":
            wait_for(ps.at[op[2], op[3], 0] if op[1] == "pr" else rl.at[op[2], op[3], 0], op)


def body(resid, norm_gains, gate_one, up_one, down_one, proj_u, proj_v, spatial, spatial_bias, mix_gain, head_gain, proj_out, gate_two, up_two, down_two):
    weights = (gate_one, up_one, down_one, proj_u, proj_v, proj_out, gate_two, up_two, down_two)
    small = (norm_gains, spatial, spatial_bias, mix_gain.reshape(1, 128), head_gain.reshape(1, 128))
    raw = (gate_one, up_one, gate_two, up_two, down_one, down_two, proj_out)
    sems_of = semaphores()
    rows, width = resid.shape
    return pl.pallas_call(
        functools.partial(kernel, sems_of),
        out_shape=jax.ShapeDtypeStruct((rows, width), BF16),
        in_specs=[pl.BlockSpec(memory_space=pltpu.HBM)] * 15,
        out_specs=pl.BlockSpec(memory_space=pltpu.VMEM),
        scratch_shapes=[pltpu.VMEM((2048, ITEMS[name][0]), BF16) for name in NAMES]
        + [
            pltpu.VMEM((3, 8, 256, 256), BF16),
            pltpu.VMEM((STREAMS, ROWS, 2048), BF16),
            pltpu.VMEM((STREAMS, ROWS, 768), BF16),
            pltpu.VMEM((3, STREAMS, 4, ROWS, 256), BF16),
            pltpu.VMEM((3, STREAMS, 4, ROWS, 256), BF16),
            pltpu.VMEM((STREAMS, 4, ROWS, 256), F32),
            pltpu.VMEM((3, STREAMS, 3, ROWS, 256), BF16),
            pltpu.VMEM((3, STREAMS, 2, HALF, 256), BF16),
            pltpu.VMEM((3, STREAMS, ROWS, 256), BF16),
            pltpu.VMEM((3, STREAMS, ROWS, 256), BF16),
            pltpu.VMEM((3, STREAMS, 2, HALF, 256), BF16),
        ]
        + [pltpu.VMEM(a.shape, a.dtype) for a in raw + small]
        + [pltpu.SemaphoreType.DMA((19,)), pltpu.SemaphoreType.DMA((len(sems_of),))],
        compiler_params=pltpu.CompilerParams(collective_id=0, has_side_effects=True, vmem_limit_bytes=60 * 2**20),
        name="layer",
    )(*weights, resid, *small)


def solution(mesh):
    in_specs = (
        P(("rep", "fs"), "tp"),
        P(),
        P("fs", "tp"),
        P("fs", "tp"),
        P("tp", "fs"),
        P("fs", "tp"),
        P("fs", "tp"),
        P("tp", None, None),
        P("tp", None),
        P("tp"),
        P("tp"),
        P("tp", "fs"),
        P("fs", "tp"),
        P("fs", "tp"),
        P("tp", "fs"),
    )
    return jax.shard_map(body, mesh=mesh, in_specs=in_specs, out_specs=P(("rep", "fs"), "tp"), check_vma=False)
```

```python
import functools
import heapq

import jax
import jax.numpy as jnp
from jax import lax
from jax.experimental import pallas as pl
from jax.experimental.pallas import tpu as pltpu
from jax.sharding import PartitionSpec as P

MESH = pl.DeviceIdType.MESH
BF16, F32 = jnp.bfloat16, jnp.float32
SHARD = 64
ITEMS = {
    "a1": (768, 48),
    "d1": (384, 48),
    "m": (512, 48),
    "a2": (768, 32),
    "b2": (640, 48),
    "d2": (640, 32),
}
NAMES = tuple(ITEMS)
SPLIT = ("a1", "d1")
TURN = {"a1": 0, "d1": 0, "m": 1, "a2": 2, "b2": 2, "d2": 2}
RATE = {"y+": 46600.0, "y-": 46600.0, "z+": 46600.0, "z-": 46600.0, "x+": 46600.0, "x-": 46600.0, "d": 250000.0, "q": 30000.0}
DELAY = {"d": 1.5}
GREET = ("y+", "y-", "z+", "z-", "x+", "x-", "d")
AHEAD = 1.5
ROWS = 128
HALF = 64
BLOCK_BYTES = ROWS * 256 * 2
STREAMS = 4
Y_FIRST, Z_FIRST, Y_SAME, Y_CROSS, Z_SAME, Z_CROSS = range(6)
TWICE_UP = (-3, -1, 1, 3)


def parts_of(name):
    return (Y_SAME, Y_CROSS, Z_SAME, Z_CROSS) if name in SPLIT else (Y_FIRST, Z_FIRST)


def y_first(part):
    return part in (Y_FIRST, Y_SAME, Y_CROSS)


def rows_of(name, part):
    return ITEMS[name][1] if y_first(part) else SHARD - ITEMS[name][1]


def needed(part, dy):
    return part in (Y_FIRST, Z_FIRST) or (dy % 2 == 0) == (part in (Y_SAME, Z_SAME))


def reach(part, dz):
    if part in (Y_SAME, Z_SAME):
        return (4, 2) if dz in (0, 2) else (2, 4)
    if part in (Y_CROSS, Z_CROSS):
        return 3, 3
    return (4, 3) if y_first(part) or dz == 2 else (3, 4)


def children(part, dy, dz):
    out = []
    up, down = reach(part, dz)
    if y_first(part):
        if dz == 0:
            if 0 <= dy < up:
                out.append(("y+", dy + 1, 0))
            if -down < dy <= 0:
                out.append(("y-", dy - 1, 0))
            if needed(part, dy):
                out += [("z+", dy, 1), ("z-", dy, -1)]
        elif dz == 1 and dy in UP[part]:
            out.append(("z+", dy, 2))
        elif dz == -1 and dy not in UP[part]:
            out.append(("z-", dy, -2))
    elif dy == 0:
        if dz == 0:
            out += [("z+", 0, 1), ("z-", 0, -1)]
        elif dz == 1 and part != Z_CROSS:
            out.append(("z+", 0, 2))
        elif dz == -1 and part == Z_CROSS:
            out.append(("z-", 0, -2))
        out += [("y+", 1, dz), ("y-", -1, dz)]
    elif 0 < dy < up:
        out.append(("y+", dy + 1, dz))
    elif -down < dy < 0:
        out.append(("y-", dy - 1, dz))
    return out


UP = {Y_FIRST: (-3, -1, 1, 3), Y_SAME: (0, 4), Y_CROSS: (-1, 1)}


def last_ones(part):
    ends = total = 0
    todo = [(0, 0)]
    while todo:
        here = todo.pop()
        after = children(part, *here)
        ends += not after
        total += 1
        todo += [(a, b) for _, a, b in after]
    return ends, total - 1


def depth(part, dy, dz):
    return max((1 + depth(part, a, b) for _, a, b in children(part, dy, dz)), default=0)


def gather_steps():
    block, half = BLOCK_BYTES, BLOCK_BYTES // 2
    return {
        "own": [("x+", block, "m1"), ("x-", block, "p1"), ("d", block, "end")],
        "m1": [("x+", half, "h0"), ("d", block, "end")],
        "p1": [("x-", half, "h1"), ("d", block, "end")],
        "h0": [("d", half, "end")],
        "h1": [("d", half, "end")],
    }


def chain(h):
    half = BLOCK_BYTES // 2
    steps = []
    for s in range(3 if h < 2 else 1):
        steps.append((("norm", s, h), [("ag", s, h)], 0.35, []))
        if s == 1:
            steps.append((("mix", s, h), [("w", "m")], 0.7, []))
        elif s == 0:
            steps.append((("gu", s, h, 0), [("w", "a1")], 0.5, []))
        else:
            for j in range(3):
                steps.append((("gu", s, h, j), [("w", "a2"), ("w", "b2")], 0.3, []))
        needs = [[("w", "d1")], [("w", "m")], [("w", "m"), ("w", "d2")]][s]
        for r in (2, 1, 3, 0):
            steps.append((("down", s, h, r, 1), needs, 0.1, [("d", BLOCK_BYTES, ("rs", s, h, "pr"), ("pr", s, h, r))]))
        for r in (2, 1, 3, 0):
            steps.append((("down", s, h, r, 0), [], 0.1, []))
        key = ("rs", s, h)
        steps.append(
            (
                ("pair", s, h),
                [key + ("pr",)],
                0.25,
                [
                    ("x+", half, key + ("l0",), ("l0", s, h)),
                    ("x-", half, key + ("l1",), ("l1", s, h)),
                    ("x+", half, key + ("ra",), ("ra1", s, h)),
                    ("x-", half, key + ("rb",), ("rb0", s, h)),
                ],
            )
        )
        steps.append((("relay0", s, h), [key + ("l0",)], 0.1, [("x+", half, key + ("ra",), ("ra0", s, h))]))
        steps.append((("relay1", s, h), [key + ("l1",)], 0.1, [("x-", half, key + ("rb",), ("rb1", s, h))]))
        waits = [key + ("ra",), key + ("rb",)]
        if h >= 2:
            steps.append((("give", s, h), waits, 0.15, [("q", BLOCK_BYTES, ("rs", 0, h - 2, "yx"), ("yx", s, h))]))
        else:
            steps.append((("end", s, h), waits + ([key + ("yx",)] if s == 0 else []), 0.2, [("next", s)]))
    return steps


SLOTS = [(s, h) for s in range(3) for h in range(2)] + [(0, 2), (0, 3)]


@functools.lru_cache(None)
def plan():
    count = {("w", name, part): last_ones(part)[0] for name in NAMES for part in parts_of(name)}
    expected = {}
    for s, h in SLOTS:
            expected[("ag", s, h)] = 5
            expected[("rs", s, h, "yx")] = 1
            expected[("rs", s, h, "pr")] = 4
            expected[("rs", s, h, "l0")] = expected[("rs", s, h, "l1")] = 1
            expected[("rs", s, h, "ra")] = expected[("rs", s, h, "rb")] = 2
    ops, now, serial = [], 0.0, 0
    free = {link: 0.0 for link in RATE}
    ready = {link: [] for link in RATE}
    arrivals, waited = [], set()

    def offer(link, priority, size, landing, op):
        nonlocal serial
        serial += 1
        heapq.heappush(ready[link], (priority, serial, size, landing, op))

    def offer_weight(index, name, part, dy, dz):
        for link, a, b in children(part, dy, dz):
            offer(
                link,
                (index, -depth(part, a, b)),
                rows_of(name, part) * ITEMS[name][0] * 2,
                ("w", index, name, part, a, b),
                ("send", name, part, dy, dz, link, a, b),
            )

    def offer_block(s, h, at):
        for link, size, landing in gather_steps()[at]:
            offer(link, (h, s), size, ("ag", s, h, landing), ("pass", s, h, at, link))

    def pump():
        nonlocal serial
        for link, queue in ready.items():
            while queue and free[link] - now < AHEAD:
                _, _, size, landing, op = heapq.heappop(queue)
                free[link] = max(free[link], now) + size / RATE[link]
                serial += 1
                heapq.heappush(arrivals, (free[link] + DELAY.get(link, 2.3), serial, landing))
                ops.append(op)

    for name in NAMES:
        for part in parts_of(name):
            offer_weight(TURN[name], name, part, 0, 0)
    for h in range(2):
        offer("q", (0, h), BLOCK_BYTES, ("ag", 0, h + 2, "own"), ("swap", h))
        offer_block(0, h, "own")
    chains = {h: chain(h) for h in (2, 3, 0, 1)}
    times = {}
    while any(chains.values()) or arrivals or any(ready.values()):
        while arrivals and arrivals[0][0] <= now:
            _, _, landing = heapq.heappop(arrivals)
            if landing[0] == "w":
                _, index, name, part, dy, dz = landing
                if children(part, dy, dz):
                    ops.append(("got", name, part, dy, dz))
                    offer_weight(index, name, part, dy, dz)
                else:
                    count[("w", name, part)] -= 1
            elif landing[0] == "ag" and landing[3] != "end":
                ops.append(("block",) + landing[1:])
                offer_block(*landing[1:])
            else:
                key = landing[:3] if landing[0] == "ag" else landing
                expected[key] -= 1
            times[landing[:3]] = now
        pump()
        ran = False
        for h, todo in chains.items():
            if not todo:
                continue
            step, needs, duration, sends = todo[0]
            done = True
            for need in needs:
                if need[0] == "w":
                    done &= all(count[("w", need[1], part)] == 0 for part in parts_of(need[1]))
                else:
                    done &= expected[need] == 0
            if not done:
                continue
            for need in needs:
                if need not in waited:
                    waited.add(need)
                    ops.append(("all",) + need)
            ops.append(("do",) + step)
            times[step] = now
            now += duration
            todo.pop(0)
            for send in sends:
                if send[0] == "next":
                    if send[1] < 2:
                        offer_block(send[1] + 1, h, "own")
                else:
                    offer(send[0], (-1, 0), send[1], send[2], ("rsend",) + send[3])
            ran = True
            break
        if ran:
            continue
        later = [arrivals[0][0]] if arrivals else []
        later += [free[link] - AHEAD + 0.01 for link, queue in ready.items() if queue]
        if not later:
            break
        now = max(min(later), now + 0.01)
    return ops, times, now


def semaphores():
    index = {}
    for name in NAMES:
        for part in parts_of(name):
            index[("all", name, part)] = len(index)
            index[("sent", name, part)] = len(index)
    for op in plan()[0]:
        if op[0] == "got":
            index[op[1:]] = len(index)
        elif op[0] in ("block", "pass", "rsend", "swap"):
            index[op] = len(index)
    for s, h in SLOTS:
        index[("ag", s, h)] = len(index)
        for what in ("pr", "l0", "l1", "ra", "rb", "yx"):
            index[("rs", s, h, what)] = len(index)
    return index


def rms_scale(values, mean_square, gain):
    return values * lax.rsqrt(mean_square + 1e-06) * gain


def contract(left, right):
    return lax.dot_general(left, right, (((1,), (1,)), ((), ())), preferred_element_type=F32)


def kernel(sems_of, *refs):
    gate_one, up_one, down_one, proj_u, proj_v, proj_out, gate_two, up_two, down_two = refs[:9]
    resid, small_in, out = refs[9], refs[10:15], refs[15]
    g = dict(zip(NAMES, refs[16:22]))
    passing = dict(zip(SPLIT, refs[22:24]))
    (xg, normed, hidden, ps, pr, po, sb, rl, ra, rb, tt, yx, yo) = refs[24:37]
    raw, small, local_sem, sems = refs[37:43], refs[43:48], refs[48], refs[49]
    gains, spatial, bias, mix_gain, head_gain = small

    rep, fs, tp = lax.axis_index("rep"), lax.axis_index("fs"), lax.axis_index("tp")
    x, core = tp // 2, tp % 2
    y, z = fs % 8, rep * 4 + fs // 8
    odd = y % 2

    def device(link):
        if link[0] == "y":
            ny = (y + (1 if link[1] == "+" else 7)) % 8
            return {"rep": rep, "fs": (fs // 8) * 8 + ny, "tp": tp}
        if link[0] == "z":
            nz = (z + (1 if link[1] == "+" else 7)) % 8
            return {"rep": nz // 4, "fs": (nz % 4) * 8 + y, "tp": tp}
        if link[0] == "x":
            nx = (x + (1 if link[1] == "+" else 3)) % 4
            return {"rep": rep, "fs": fs, "tp": nx * 2 + core}
        if link == "q":
            return {"rep": rep, "fs": fs + 1 - 2 * odd, "tp": tp}
        return {"rep": rep, "fs": fs, "tp": x * 2 + 1 - core}

    devices = {link: device(link) for link in RATE}
    barrier = pltpu.get_barrier_semaphore()
    for link in GREET:
        pl.semaphore_signal(barrier, inc=1, device_id=devices[link], device_id_type=MESH)

    own = pl.multiple_of(fs * SHARD, SHARD)
    rows = pl.ds(own, SHARD)
    pairs = []
    for which, side in ((g, odd), (passing, 1 - odd)):
        main = pl.ds(pl.multiple_of(side * 256, 256), 256)
        pairs += [
            (gate_one.at[:, main], which["a1"].at[rows, pl.ds(0, 256)]),
            (up_one.at[:, main], which["a1"].at[rows, pl.ds(384, 256)]),
            (down_one.at[:, main], which["d1"].at[rows, pl.ds(0, 256)]),
        ]
    pairs += [
        (up_two.at[:, pl.ds(0, 640)], g["b2"].at[rows]),
        (gate_two.at[:, pl.ds(0, 640)], g["a2"].at[rows, pl.ds(0, 640)]),
        (down_two.at[:, pl.ds(0, 640)], g["d2"].at[rows]),
        (proj_out, g["m"].at[rows, pl.ds(256, 128)]),
        (proj_u, g["m"].at[rows, pl.ds(0, 128)]),
        (proj_v, g["m"].at[rows, pl.ds(128, 128)]),
        (resid, xg.at[0, tp]),
    ]
    first_copies = len(pairs)
    pairs += list(zip((gate_one, up_one, gate_two, up_two, down_one, down_two), raw))
    pairs += list(zip(small_in, small))
    copies = [pltpu.make_async_copy(src, dst, local_sem.at[k]) for k, (src, dst) in enumerate(pairs)]
    for copy in copies[first_copies:] + copies[:first_copies]:
        copy.start()
    for copy in copies[first_copies:]:
        copy.wait()
    empty = jnp.zeros((SHARD, 64), BF16)
    for name, column, k in (("a1", 256, 0), ("a1", 640, 1), ("d1", 256, 4)):
        low = raw[k][:, 512:640]
        high = jnp.concatenate([raw[k][:, 640:704], empty], axis=1)
        g[name][rows, column : column + 128] = jnp.where(odd == 0, low, high)
        passing[name][rows, column : column + 128] = jnp.where(odd == 0, high, low)
    g["a2"][rows, 640:768] = jnp.concatenate([raw[3][:, 640:704], raw[2][:, 640:704]], axis=1)
    g["m"][rows, 384:512] = jnp.concatenate([empty, raw[5][:, 640:704]], axis=1)
    pl.semaphore_wait(barrier, len(GREET))
    for copy in copies[:first_copies]:
        copy.wait()

    def piece(name, part, dy, dz, at=None):
        f = ((z + 8 - dz) % 4) * 8 + (y + 8 - dy) % 8
        start = f * SHARD + (0 if y_first(part) else ITEMS[name][1])
        array = g[name] if needed(part, dy if at is None else at) else passing[name]
        return array.at[pl.ds(pl.multiple_of(start, 16), rows_of(name, part))]

    def remote(src, dst, send, recv, link):
        return pltpu.make_async_remote_copy(
            src_ref=src,
            dst_ref=dst,
            send_sem=sems.at[sems_of[send]],
            recv_sem=sems.at[sems_of[recv]],
            device_id=devices[link],
            device_id_type=MESH,
        )

    def wait_for(ref, key):
        pltpu.make_async_copy(ref, ref, sems.at[sems_of[key]]).wait()

    def block_at(s, h, at):
        shift = {"own": 0, "m1": 3, "p1": 1, "h0": 2, "h1": 2}[at]
        start, size = (h % 2) * ROWS, ROWS
        if at[0] == "h":
            start, size = start + (0 if at == "h0" else HALF), HALF
        return xg.at[3 if h >= 2 else s, ((x + shift) % 4) * 2 + core, pl.ds(start, size)]

    def slot(s, h):
        return SLOTS.index((s, h))

    def down(s, h, r, other):
        t = ((x + r) % 4) * 2 + (1 - core if other else core)
        at = pl.ds(pl.multiple_of(t * 256, 256), 256)
        if s == 1:
            total = contract(hidden[h, :, :128], g["m"][at, 256:384])
        elif s == 0:
            total = contract(hidden[h, :, :384], g["d1"][at, :])
        else:
            total = contract(hidden[h, :, :640], g["d2"][at, :])
            total = total + contract(hidden[h, :, 640:768], g["m"][at, 384:512])
        if other:
            ps[slot(s, h), r] = total.astype(BF16)
        else:
            po[h, r] = total

    def gate_up(s, h, j):
        if s == 0:
            gate = jnp.dot(normed[h], g["a1"][:, 0:384], preferred_element_type=F32)
            up = jnp.dot(normed[h], g["a1"][:, 384:768], preferred_element_type=F32)
            hidden[h, :, :384] = (jax.nn.silu(gate) * up).astype(BF16)
            return
        a, b = g["a2"], g["b2"]
        first = jnp.dot(normed[h], a[:, 256 * j : 256 * (j + 1)], preferred_element_type=F32)
        if j < 2:
            second = jnp.dot(normed[h], b[:, 256 * j : 256 * (j + 1)], preferred_element_type=F32)
            hidden[h, :, 256 * j : 256 * (j + 1)] = (jax.nn.silu(first) * second).astype(BF16)
            return
        second = jnp.dot(normed[h], b[:, 512:640], preferred_element_type=F32)
        hidden[h, :, 512:640] = (jax.nn.silu(first[:, :128]) * second).astype(BF16)
        rest = first[:, 128:]
        value = jax.nn.silu(rest) * pltpu.roll(rest, 64, 1)
        lane = lax.broadcasted_iota(jnp.int32, (ROWS, 128), 1)
        hidden[h, :, 640:768] = jnp.where(lane >= 64, value, 0.0).astype(BF16)

    def norm(s, h):
        rows = slice((h % 2) * ROWS, (h % 2 + 1) * ROWS)
        stage, s = s, 3 if h >= 2 else s
        total = jnp.zeros((ROWS, 1), F32)
        for t in range(8):
            values = xg[s, t, rows].astype(F32)
            total = total + jnp.sum(values * values, axis=-1, keepdims=True)
        for t in range(8):
            cols = slice(256 * t, 256 * (t + 1))
            scaled = rms_scale(xg[s, t, rows].astype(F32), total / 2048.0, gains[stage : stage + 1, cols])
            normed[h, :, cols] = scaled.astype(BF16)

    def mix(h):
        both = jnp.dot(normed[h], g["m"][:, 0:256], preferred_element_type=F32)
        u, v = jax.nn.gelu(both[:, :128]), jax.nn.gelu(both[:, 128:])
        centre = jnp.mean(v, axis=-1, keepdims=True)
        spread = jnp.mean(jnp.square(v - centre), axis=-1, keepdims=True)
        vn = ((v - centre) * lax.rsqrt(spread + 1e-05) * mix_gain[...]).astype(BF16)
        to, source = lax.broadcasted_iota(jnp.int32, (128, 128), 0), lax.broadcasted_iota(jnp.int32, (128, 128), 1)
        masked = jnp.where(to // 64 >= source // 64, spatial[0].astype(F32), 0.0).astype(BF16)
        offset = jnp.sum(jnp.where(to == source, bias[...], 0.0), axis=-1, keepdims=True)
        product = u * (jnp.dot(masked, vn, preferred_element_type=F32) + offset)
        square = jnp.mean(product * product, axis=-1, keepdims=True)
        hidden[h, :, :128] = rms_scale(product, square, head_gain[...]).astype(BF16)

    lower, upper = pl.ds(0, HALF), pl.ds(HALF, HALF)
    for op in plan()[0]:
        kind = op[0]
        if kind == "send":
            _, name, part, dy, dz, link, a, b = op
            landing = (name, part, a, b) if children(part, a, b) else ("all", name, part)
            remote(piece(name, part, dy, dz), piece(name, part, dy, dz, a), ("sent", name, part), landing, link).start()
        elif kind == "swap":
            h = op[1]
            src, dst = xg.at[0, tp, pl.ds(h * ROWS, ROWS)], xg.at[3, tp, pl.ds(h * ROWS, ROWS)]
            remote(src, dst, op, ("block", 0, h + 2, "own"), "q").start()
        elif kind == "got":
            _, name, part, dy, dz = op
            wait_for(piece(name, part, dy, dz), op[1:])
        elif kind == "pass":
            _, s, h, at, link = op
            ref = block_at(s, h, at)
            if link == "d":
                landing = ("ag", s, h)
            else:
                arrived = {"own": {"x+": "m1", "x-": "p1"}, "m1": {"x+": "h0"}, "p1": {"x-": "h1"}}[at][link]
                landing = ("block", s, h, arrived)
                if at == "m1":
                    ref = ref.at[lower]
                elif at == "p1":
                    ref = ref.at[upper]
            remote(ref, ref, op, landing, link).start()
        elif kind == "block":
            wait_for(block_at(*op[1:]), op)
        elif kind == "rsend":
            what, s, h = op[1:4]
            key, k = ("rs", s, h), slot(s, h)
            if what == "pr":
                remote(ps.at[k, op[4]], pr.at[k, op[4]], op, key + ("pr",), "d").start()
            elif what == "l0":
                remote(sb.at[k, 1, lower], rl.at[k, 0], op, key + ("l0",), "x+").start()
            elif what == "l1":
                remote(sb.at[k, 1, upper], rl.at[k, 1], op, key + ("l1",), "x-").start()
            elif what == "ra1":
                remote(sb.at[k, 0, upper], ra.at[k, upper], op, key + ("ra",), "x+").start()
            elif what == "rb0":
                remote(sb.at[k, 2, lower], rb.at[k, lower], op, key + ("rb",), "x-").start()
            elif what == "ra0":
                remote(tt.at[k, 0], ra.at[k, lower], op, key + ("ra",), "x+").start()
            elif what == "rb1":
                remote(tt.at[k, 1], rb.at[k, upper], op, key + ("rb",), "x-").start()
            elif what == "yx":
                remote(yo.at[h - 2], yx.at[h - 2], op, ("rs", 0, h - 2, "yx"), "q").start()
        elif kind == "all":
            if op[1] == "w":
                name = op[2]
                for part in parts_of(name):
                    many = last_ones(part)[0] * rows_of(name, part)
                    wait_for(g[name].at[pl.ds(0, many)], ("all", name, part))
            elif op[1] == "ag":
                wait_for(xg.at[op[2], pl.ds(0, 4), pl.ds(0, ROWS)], op[1:])
            else:
                _, _, s, h, what = op
                k = slot(s, h)
                at = {"pr": pr.at[k], "l0": rl.at[k, 0], "l1": rl.at[k, 1], "ra": ra.at[k], "rb": rb.at[k], "yx": yx.at[h % 2]}
                wait_for(at[what], op[1:])
        else:
            what, s, h = op[1:4]
            k = slot(s, h)
            if what == "norm":
                norm(s, h)
            elif what == "gu":
                gate_up(s, h, op[4])
            elif what == "mix":
                mix(h)
            elif what == "down":
                down(s, h, op[4], op[5])
            elif what == "pair":
                po[h, 0] = po[h, 0] + pr[k, 0].astype(F32)
                for r in (2, 1, 3):
                    sb[k, r - 1] = (po[h, r] + pr[k, r].astype(F32)).astype(BF16)
            elif what == "relay0":
                tt[k, 0] = (sb[k, 0, :HALF].astype(F32) + rl[k, 0].astype(F32)).astype(BF16)
            elif what == "relay1":
                tt[k, 1] = (sb[k, 2, HALF:].astype(F32) + rl[k, 1].astype(F32)).astype(BF16)
            else:
                total = po[h, 0] + ra[k].astype(F32) + rb[k].astype(F32)
                if what == "give":
                    yo[h - 2] = total.astype(BF16)
                    continue
                if s == 0:
                    total = total + yx[h].astype(F32)
                at = slice(h * ROWS, (h + 1) * ROWS)
                value = (xg[s, tp, at].astype(F32) + (1.0 if s == 1 else 0.5) * total).astype(BF16)
                if s < 2:
                    xg[s + 1, tp, at] = value
                else:
                    out[at, :] = value

    for name in NAMES:
        for part in parts_of(name):
            wait_for(g[name].at[pl.ds(0, last_ones(part)[1] * rows_of(name, part))], ("sent", name, part))
    for op in plan()[0]:
        if op[0] == "pass":
            ref = block_at(op[1], op[2], op[3])
            if op[3] in ("m1", "p1") and op[4] != "d":
                ref = ref.at[lower]
            wait_for(ref, op)
        elif op[0] == "rsend":
            wait_for(ps.at[0, 0] if op[1] in ("pr", "yx") else rl.at[0, 0], op)
        elif op[0] == "swap":
            wait_for(ps.at[0, 0], op)


def body(resid, norm_gains, gate_one, up_one, down_one, proj_u, proj_v, spatial, spatial_bias, mix_gain, head_gain, proj_out, gate_two, up_two, down_two):
    weights = (gate_one, up_one, down_one.T, proj_u, proj_v, proj_out.T, gate_two, up_two, down_two.T)
    small = (norm_gains, spatial, spatial_bias, mix_gain.reshape(1, 128), head_gain.reshape(1, 128))
    raw = (gate_one, up_one, gate_two, up_two, down_one.T, down_two.T)
    sems_of = semaphores()
    rows, width = resid.shape
    return pl.pallas_call(
        functools.partial(kernel, sems_of),
        out_shape=jax.ShapeDtypeStruct((rows, width), BF16),
        in_specs=[pl.BlockSpec(memory_space=pltpu.HBM)] * 15,
        out_specs=pl.BlockSpec(memory_space=pltpu.VMEM),
        scratch_shapes=[pltpu.VMEM((2048, ITEMS[name][0]), BF16) for name in NAMES]
        + [pltpu.VMEM((2048, ITEMS[name][0]), BF16) for name in SPLIT]
        + [
            pltpu.VMEM((4, 8, 256, 256), BF16),
            pltpu.VMEM((STREAMS, ROWS, 2048), BF16),
            pltpu.VMEM((STREAMS, ROWS, 768), BF16),
            pltpu.VMEM((8, 4, ROWS, 256), BF16),
            pltpu.VMEM((8, 4, ROWS, 256), BF16),
            pltpu.VMEM((STREAMS, 4, ROWS, 256), F32),
            pltpu.VMEM((8, 3, ROWS, 256), BF16),
            pltpu.VMEM((8, 2, HALF, 256), BF16),
            pltpu.VMEM((8, ROWS, 256), BF16),
            pltpu.VMEM((8, ROWS, 256), BF16),
            pltpu.VMEM((8, 2, HALF, 256), BF16),
            pltpu.VMEM((2, ROWS, 256), BF16),
            pltpu.VMEM((2, ROWS, 256), BF16),
        ]
        + [pltpu.VMEM(a.shape, a.dtype) for a in raw + small]
        + [pltpu.SemaphoreType.DMA((24,)), pltpu.SemaphoreType.DMA((len(sems_of),))],
        compiler_params=pltpu.CompilerParams(collective_id=0, has_side_effects=True, vmem_limit_bytes=60 * 2**20),
        name="layer",
    )(*weights, resid, *small)


def solution(mesh):
    in_specs = (
        P(("rep", "fs"), "tp"),
        P(),
        P("fs", "tp"),
        P("fs", "tp"),
        P("tp", "fs"),
        P("fs", "tp"),
        P("fs", "tp"),
        P("tp", None, None),
        P("tp", None),
        P("tp"),
        P("tp"),
        P("tp", "fs"),
        P("fs", "tp"),
        P("fs", "tp"),
        P("tp", "fs"),
    )
    return jax.shard_map(body, mesh=mesh, in_specs=in_specs, out_specs=P(("rep", "fs"), "tp"), check_vma=False)
```

```python
import functools
import heapq

import jax
import jax.numpy as jnp
from jax import lax
from jax.experimental import pallas as pl
from jax.experimental.pallas import tpu as pltpu
from jax.sharding import PartitionSpec as P

MESH = pl.DeviceIdType.MESH
BF16, F32 = jnp.bfloat16, jnp.float32
SHARD = 64
ITEMS = {
    "f1": (1152, 48),
    "m": (512, 48),
    "f2a": (1024, 32),
    "f2b": (1024, 48),
}
NAMES = tuple(ITEMS)
SPLIT = ("f1",)
TURN = {"f1": 0, "m": 1, "f2a": 2, "f2b": 2}
RATE = {"y+": 46600.0, "y-": 46600.0, "z+": 46600.0, "z-": 46600.0, "x+": 46600.0, "x-": 46600.0, "d": 250000.0, "q": 30000.0}
DELAY = {"d": 1.5}
GREET = ("y+", "y-", "z+", "z-", "x+", "x-", "d")
AHEAD = 1.5
LEAST = 0.5
ROWS = 128
HALF = 64
BLOCK_BYTES = ROWS * 256 * 2
STREAMS = 4
Y_FIRST, Z_FIRST, Y_SAME, Y_CROSS, Z_SAME, Z_CROSS = range(6)
TWICE_UP = (-3, -1, 1, 3)


def parts_of(name):
    return (Y_SAME, Y_CROSS, Z_SAME, Z_CROSS) if name in SPLIT else (Y_FIRST, Z_FIRST)


def y_first(part):
    return part in (Y_FIRST, Y_SAME, Y_CROSS)


def rows_of(name, part):
    return ITEMS[name][1] if y_first(part) else SHARD - ITEMS[name][1]


def needed(part, dy):
    return part in (Y_FIRST, Z_FIRST) or (dy % 2 == 0) == (part in (Y_SAME, Z_SAME))


def reach(part, dz):
    if part in (Y_SAME, Z_SAME):
        return (4, 2) if dz in (0, 2) else (2, 4)
    if part in (Y_CROSS, Z_CROSS):
        return 3, 3
    return (4, 3) if y_first(part) or dz == 2 else (3, 4)


def children(part, dy, dz):
    out = []
    up, down = reach(part, dz)
    if y_first(part):
        if dz == 0:
            if 0 <= dy < up:
                out.append(("y+", dy + 1, 0))
            if -down < dy <= 0:
                out.append(("y-", dy - 1, 0))
            if needed(part, dy):
                out += [("z+", dy, 1), ("z-", dy, -1)]
        elif dz == 1 and dy in UP[part]:
            out.append(("z+", dy, 2))
        elif dz == -1 and dy not in UP[part]:
            out.append(("z-", dy, -2))
    elif dy == 0:
        if dz == 0:
            out += [("z+", 0, 1), ("z-", 0, -1)]
        elif dz == 1 and part != Z_CROSS:
            out.append(("z+", 0, 2))
        elif dz == -1 and part == Z_CROSS:
            out.append(("z-", 0, -2))
        out += [("y+", 1, dz), ("y-", -1, dz)]
    elif 0 < dy < up:
        out.append(("y+", dy + 1, dz))
    elif -down < dy < 0:
        out.append(("y-", dy - 1, dz))
    return out


UP = {Y_FIRST: (-3, -1, 1, 3), Y_SAME: (0, 4), Y_CROSS: (-1, 1)}


def last_ones(part):
    ends = total = 0
    todo = [(0, 0)]
    while todo:
        here = todo.pop()
        after = children(part, *here)
        ends += not after
        total += 1
        todo += [(a, b) for _, a, b in after]
    return ends, total - 1


def depth(part, dy, dz):
    return max((1 + depth(part, a, b) for _, a, b in children(part, dy, dz)), default=0)


def gather_steps():
    block, half = BLOCK_BYTES, BLOCK_BYTES // 2
    return {
        "own": [("x+", block, "m1"), ("x-", block, "p1"), ("d", block, "end")],
        "m1": [("x+", half, "h0"), ("d", block, "end")],
        "p1": [("x-", half, "h1"), ("d", block, "end")],
        "h0": [("d", half, "end")],
        "h1": [("d", half, "end")],
    }


def chain(h):
    half = BLOCK_BYTES // 2
    steps = []
    for s in range(3 if h < 2 else 1):
        steps.append((("norm", s, h), [("ag", s, h)], 0.35, []))
        if s == 1:
            steps.append((("mix", s, h), [("w", "m")], 0.7, []))
        elif s == 0:
            steps.append((("gu", s, h, 0), [("w", "f1")], 0.5, []))
        else:
            for j in range(3):
                steps.append((("gu", s, h, j), [("w", "f2a"), ("w", "f2b")], 0.3, []))
        needs = [[("w", "f1")], [("w", "m")], [("w", "m"), ("w", "f2b")]][s]
        for r in (2, 1, 3, 0):
            steps.append((("down", s, h, r, 1), needs, 0.1, [("d", BLOCK_BYTES, ("rs", s, h, "pr"), ("pr", s, h, r))]))
        for r in (2, 1, 3, 0):
            steps.append((("down", s, h, r, 0), [], 0.1, []))
        key = ("rs", s, h)
        steps.append(
            (
                ("pair", s, h),
                [key + ("pr",)],
                0.25,
                [
                    ("x+", half, key + ("l0",), ("l0", s, h)),
                    ("x-", half, key + ("l1",), ("l1", s, h)),
                    ("x+", half, key + ("ra",), ("ra1", s, h)),
                    ("x-", half, key + ("rb",), ("rb0", s, h)),
                ],
            )
        )
        steps.append((("relay0", s, h), [key + ("l0",)], 0.1, [("x+", half, key + ("ra",), ("ra0", s, h))]))
        steps.append((("relay1", s, h), [key + ("l1",)], 0.1, [("x-", half, key + ("rb",), ("rb1", s, h))]))
        waits = [key + ("ra",), key + ("rb",)]
        if h >= 2:
            steps.append((("give", s, h), waits, 0.15, [("q", BLOCK_BYTES, ("rs", 0, h - 2, "yx"), ("yx", s, h))]))
        else:
            steps.append((("end", s, h), waits + ([key + ("yx",)] if s == 0 else []), 0.2, [("next", s)]))
    return steps


SLOTS = [(s, h) for s in range(3) for h in range(2)] + [(0, 2), (0, 3)]


@functools.lru_cache(None)
def plan():
    count = {("w", name, part): last_ones(part)[0] for name in NAMES for part in parts_of(name)}
    expected = {}
    for s, h in SLOTS:
            expected[("ag", s, h)] = 5
            expected[("rs", s, h, "yx")] = 1
            expected[("rs", s, h, "pr")] = 4
            expected[("rs", s, h, "l0")] = expected[("rs", s, h, "l1")] = 1
            expected[("rs", s, h, "ra")] = expected[("rs", s, h, "rb")] = 2
    ops, now, serial = [], 0.0, 0
    free = {link: 0.0 for link in RATE}
    ready = {link: [] for link in RATE}
    arrivals, waited = [], set()

    def offer(link, priority, size, landing, op):
        nonlocal serial
        serial += 1
        heapq.heappush(ready[link], (priority, serial, size, landing, op))

    def offer_weight(index, name, part, dy, dz):
        for link, a, b in children(part, dy, dz):
            offer(
                link,
                (index, -depth(part, a, b)),
                rows_of(name, part) * ITEMS[name][0] * 2,
                ("w", index, name, part, a, b),
                ("send", name, part, dy, dz, link, a, b),
            )

    def offer_block(s, h, at):
        for link, size, landing in gather_steps()[at]:
            offer(link, (h, s), size, ("ag", s, h, landing), ("pass", s, h, at, link))

    def pump():
        nonlocal serial
        for link, queue in ready.items():
            while queue and free[link] - now < AHEAD:
                _, _, size, landing, op = heapq.heappop(queue)
                free[link] = max(free[link], now) + max(size / RATE[link], LEAST)
                if link == "q":
                    for shared in ("y+", "y-"):
                        free[shared] = max(free[shared], now) + 0.5 * size / RATE[shared]
                serial += 1
                heapq.heappush(arrivals, (free[link] + DELAY.get(link, 2.3), serial, landing))
                ops.append(op)

    for name in NAMES:
        for part in parts_of(name):
            offer_weight(TURN[name], name, part, 0, 0)
    for h in range(2):
        offer("q", (0, h), BLOCK_BYTES, ("ag", 0, h + 2, "own"), ("swap", h))
        offer_block(0, h, "own")
    chains = {h: chain(h) for h in (2, 3, 0, 1)}
    times = {}
    while any(chains.values()) or arrivals or any(ready.values()):
        while arrivals and arrivals[0][0] <= now:
            _, _, landing = heapq.heappop(arrivals)
            if landing[0] == "w":
                _, index, name, part, dy, dz = landing
                if children(part, dy, dz):
                    ops.append(("got", name, part, dy, dz))
                    offer_weight(index, name, part, dy, dz)
                else:
                    count[("w", name, part)] -= 1
            elif landing[0] == "ag" and landing[3] != "end":
                ops.append(("block",) + landing[1:])
                offer_block(*landing[1:])
            else:
                key = landing[:3] if landing[0] == "ag" else landing
                expected[key] -= 1
            times[landing[:3]] = now
        pump()
        ran = False
        for h, todo in chains.items():
            if not todo:
                continue
            step, needs, duration, sends = todo[0]
            done = True
            for need in needs:
                if need[0] == "w":
                    done &= all(count[("w", need[1], part)] == 0 for part in parts_of(need[1]))
                else:
                    done &= expected[need] == 0
            if not done:
                continue
            for need in needs:
                if need not in waited:
                    waited.add(need)
                    ops.append(("all",) + need)
            ops.append(("do",) + step)
            times[step] = now
            now += 0.6 * duration
            todo.pop(0)
            for send in sends:
                if send[0] == "next":
                    if send[1] < 2:
                        offer_block(send[1] + 1, h, "own")
                else:
                    offer(send[0], (-1, 0), send[1], send[2], ("rsend",) + send[3])
            ran = True
            break
        if ran:
            continue
        later = [arrivals[0][0]] if arrivals else []
        later += [free[link] - AHEAD + 0.01 for link, queue in ready.items() if queue]
        if not later:
            break
        now = max(min(later), now + 0.01)
    return ops, times, now


def semaphores():
    index = {}
    for name in NAMES:
        for part in parts_of(name):
            index[("all", name, part)] = len(index)
            index[("sent", name, part)] = len(index)
    for op in plan()[0]:
        if op[0] == "got":
            index[op[1:]] = len(index)
        elif op[0] in ("block", "pass", "rsend", "swap"):
            index[op] = len(index)
    for s, h in SLOTS:
        index[("ag", s, h)] = len(index)
        for what in ("pr", "l0", "l1", "ra", "rb", "yx"):
            index[("rs", s, h, what)] = len(index)
    return index


def rms_scale(values, mean_square, gain):
    return values * lax.rsqrt(mean_square + 1e-06) * gain


def contract(left, right):
    return lax.dot_general(left, right, (((1,), (1,)), ((), ())), preferred_element_type=F32)


def kernel(sems_of, *refs):
    gate_one, up_one, down_one, proj_u, proj_v, proj_out, gate_two, up_two, down_two = refs[:9]
    resid, small_in, out = refs[9], refs[10:15], refs[15]
    g = dict(zip(NAMES, refs[16:20]))
    passing = {"f1": refs[20]}
    (xg, normed, hidden, ps, pr, po, sb, rl, ra, rb, tt, yx, yo) = refs[21:34]
    raw, small, local_sem, sems = refs[34:40], refs[40:45], refs[45], refs[46]
    gains, spatial, bias, mix_gain, head_gain = small

    rep, fs, tp = lax.axis_index("rep"), lax.axis_index("fs"), lax.axis_index("tp")
    x, core = tp // 2, tp % 2
    y, z = fs % 8, rep * 4 + fs // 8
    odd = y % 2

    def device(link):
        if link[0] == "y":
            ny = (y + (1 if link[1] == "+" else 7)) % 8
            return {"rep": rep, "fs": (fs // 8) * 8 + ny, "tp": tp}
        if link[0] == "z":
            nz = (z + (1 if link[1] == "+" else 7)) % 8
            return {"rep": nz // 4, "fs": (nz % 4) * 8 + y, "tp": tp}
        if link[0] == "x":
            nx = (x + (1 if link[1] == "+" else 3)) % 4
            return {"rep": rep, "fs": fs, "tp": nx * 2 + core}
        if link == "q":
            return {"rep": rep, "fs": fs + 1 - 2 * odd, "tp": tp}
        return {"rep": rep, "fs": fs, "tp": x * 2 + 1 - core}

    devices = {link: device(link) for link in RATE}
    barrier = pltpu.get_barrier_semaphore()
    for link in GREET:
        pl.semaphore_signal(barrier, inc=1, device_id=devices[link], device_id_type=MESH)

    own = pl.multiple_of(fs * SHARD, SHARD)
    rows = pl.ds(own, SHARD)
    early = [(resid, xg.at[0, tp])] + list(zip((gate_one, up_one, down_one), raw[:3]))
    for array, side in ((g["f1"], odd), (passing["f1"], 1 - odd)):
        main = pl.ds(pl.multiple_of(side * 256, 256), 256)
        early += [(w.at[:, main], array.at[rows, pl.ds(384 * k, 256)]) for k, w in enumerate((gate_one, up_one, down_one))]
    late = list(zip((gate_two, up_two, down_two), raw[3:])) + [
        (proj_u, g["m"].at[rows, pl.ds(0, 128)]),
        (proj_v, g["m"].at[rows, pl.ds(128, 128)]),
        (proj_out, g["m"].at[rows, pl.ds(256, 128)]),
        (gate_two.at[:, pl.ds(0, 640)], g["f2a"].at[rows, pl.ds(0, 640)]),
        (down_two.at[:, pl.ds(0, 256)], g["f2a"].at[rows, pl.ds(768, 256)]),
        (up_two.at[:, pl.ds(0, 640)], g["f2b"].at[rows, pl.ds(0, 640)]),
        (down_two.at[:, pl.ds(256, 384)], g["f2b"].at[rows, pl.ds(640, 384)]),
    ]
    late += list(zip(small_in, small))
    copies = [pltpu.make_async_copy(src, dst, local_sem.at[k]) for k, (src, dst) in enumerate(early + late)]
    for copy in copies:
        copy.start()
    empty = jnp.zeros((SHARD, 64), BF16)
    for copy in copies[: len(early)]:
        copy.wait()
    for k in range(3):
        low = raw[k][:, 512:640]
        high = jnp.concatenate([raw[k][:, 640:704], empty], axis=1)
        column = 384 * k + 256
        g["f1"][rows, column : column + 128] = jnp.where(odd == 0, low, high)
        passing["f1"][rows, column : column + 128] = jnp.where(odd == 0, high, low)
    pl.semaphore_wait(barrier, len(GREET))

    def prepare_rest():
        for copy in copies[len(early) :]:
            copy.wait()
        g["f2a"][rows, 640:768] = jnp.concatenate([raw[4][:, 640:704], raw[3][:, 640:704]], axis=1)
        g["m"][rows, 384:512] = jnp.concatenate([empty, raw[5][:, 640:704]], axis=1)

    def piece(name, part, dy, dz, at=None):
        f = ((z + 8 - dz) % 4) * 8 + (y + 8 - dy) % 8
        start = f * SHARD + (0 if y_first(part) else ITEMS[name][1])
        array = g[name] if needed(part, dy if at is None else at) else passing[name]
        return array.at[pl.ds(pl.multiple_of(start, 16), rows_of(name, part))]

    def remote(src, dst, send, recv, link):
        return pltpu.make_async_remote_copy(
            src_ref=src,
            dst_ref=dst,
            send_sem=sems.at[sems_of[send]],
            recv_sem=sems.at[sems_of[recv]],
            device_id=devices[link],
            device_id_type=MESH,
        )

    def wait_for(ref, key):
        pltpu.make_async_copy(ref, ref, sems.at[sems_of[key]]).wait()

    def block_at(s, h, at):
        shift = {"own": 0, "m1": 3, "p1": 1, "h0": 2, "h1": 2}[at]
        start, size = (h % 2) * ROWS, ROWS
        if at[0] == "h":
            start, size = start + (0 if at == "h0" else HALF), HALF
        return xg.at[3 if h >= 2 else s, ((x + shift) % 4) * 2 + core, pl.ds(start, size)]

    def slot(s, h):
        return SLOTS.index((s, h))

    def down(s, h, r, other):
        t = ((x + r) % 4) * 2 + (1 - core if other else core)
        at = pl.ds(pl.multiple_of(t * 256, 256), 256)
        if s == 1:
            total = contract(hidden[h, :, :128], g["m"][at, 256:384])
        elif s == 0:
            total = contract(hidden[h, :, :384], g["f1"][at, 768:1152])
        else:
            total = contract(hidden[h, :, :256], g["f2a"][at, 768:1024])
            total = total + contract(hidden[h, :, 256:640], g["f2b"][at, 640:1024])
            total = total + contract(hidden[h, :, 640:768], g["m"][at, 384:512])
        if other:
            ps[slot(s, h), r] = total.astype(BF16)
        else:
            po[h, r] = total

    def gate_up(s, h, j):
        if s == 0:
            gate = jnp.dot(normed[h], g["f1"][:, 0:384], preferred_element_type=F32)
            up = jnp.dot(normed[h], g["f1"][:, 384:768], preferred_element_type=F32)
            hidden[h, :, :384] = (jax.nn.silu(gate) * up).astype(BF16)
            return
        a, b = g["f2a"], g["f2b"]
        first = jnp.dot(normed[h], a[:, 256 * j : 256 * (j + 1)], preferred_element_type=F32)
        if j < 2:
            second = jnp.dot(normed[h], b[:, 256 * j : 256 * (j + 1)], preferred_element_type=F32)
            hidden[h, :, 256 * j : 256 * (j + 1)] = (jax.nn.silu(first) * second).astype(BF16)
            return
        second = jnp.dot(normed[h], b[:, 512:640], preferred_element_type=F32)
        hidden[h, :, 512:640] = (jax.nn.silu(first[:, :128]) * second).astype(BF16)
        rest = first[:, 128:]
        value = jax.nn.silu(rest) * pltpu.roll(rest, 64, 1)
        lane = lax.broadcasted_iota(jnp.int32, (ROWS, 128), 1)
        hidden[h, :, 640:768] = jnp.where(lane >= 64, value, 0.0).astype(BF16)

    def norm(s, h):
        rows = slice((h % 2) * ROWS, (h % 2 + 1) * ROWS)
        stage, s = s, 3 if h >= 2 else s
        total = jnp.zeros((ROWS, 1), F32)
        for t in range(8):
            values = xg[s, t, rows].astype(F32)
            total = total + jnp.sum(values * values, axis=-1, keepdims=True)
        for t in range(8):
            cols = slice(256 * t, 256 * (t + 1))
            scaled = rms_scale(xg[s, t, rows].astype(F32), total / 2048.0, gains[stage : stage + 1, cols])
            normed[h, :, cols] = scaled.astype(BF16)

    def mix(h):
        both = jnp.dot(normed[h], g["m"][:, 0:256], preferred_element_type=F32)
        u, v = jax.nn.gelu(both[:, :128]), jax.nn.gelu(both[:, 128:])
        centre = jnp.mean(v, axis=-1, keepdims=True)
        spread = jnp.mean(jnp.square(v - centre), axis=-1, keepdims=True)
        vn = ((v - centre) * lax.rsqrt(spread + 1e-05) * mix_gain[...]).astype(BF16)
        to, source = lax.broadcasted_iota(jnp.int32, (128, 128), 0), lax.broadcasted_iota(jnp.int32, (128, 128), 1)
        masked = jnp.where(to // 64 >= source // 64, spatial[0].astype(F32), 0.0).astype(BF16)
        offset = jnp.sum(jnp.where(to == source, bias[...], 0.0), axis=-1, keepdims=True)
        product = u * (jnp.dot(masked, vn, preferred_element_type=F32) + offset)
        square = jnp.mean(product * product, axis=-1, keepdims=True)
        hidden[h, :, :128] = rms_scale(product, square, head_gain[...]).astype(BF16)

    lower, upper = pl.ds(0, HALF), pl.ds(HALF, HALF)
    prepared = False
    for op in plan()[0]:
        kind = op[0]
        if not prepared and (kind == "got" or (kind == "send" and op[1] != "f1") or kind in ("all", "do")):
            prepared = True
            prepare_rest()
        if kind == "send":
            _, name, part, dy, dz, link, a, b = op
            landing = (name, part, a, b) if children(part, a, b) else ("all", name, part)
            remote(piece(name, part, dy, dz), piece(name, part, dy, dz, a), ("sent", name, part), landing, link).start()
        elif kind == "swap":
            h = op[1]
            src, dst = xg.at[0, tp, pl.ds(h * ROWS, ROWS)], xg.at[3, tp, pl.ds(h * ROWS, ROWS)]
            remote(src, dst, op, ("block", 0, h + 2, "own"), "q").start()
        elif kind == "got":
            _, name, part, dy, dz = op
            wait_for(piece(name, part, dy, dz), op[1:])
        elif kind == "pass":
            _, s, h, at, link = op
            ref = block_at(s, h, at)
            if link == "d":
                landing = ("ag", s, h)
            else:
                arrived = {"own": {"x+": "m1", "x-": "p1"}, "m1": {"x+": "h0"}, "p1": {"x-": "h1"}}[at][link]
                landing = ("block", s, h, arrived)
                if at == "m1":
                    ref = ref.at[lower]
                elif at == "p1":
                    ref = ref.at[upper]
            remote(ref, ref, op, landing, link).start()
        elif kind == "block":
            wait_for(block_at(*op[1:]), op)
        elif kind == "rsend":
            what, s, h = op[1:4]
            key, k = ("rs", s, h), slot(s, h)
            if what == "pr":
                remote(ps.at[k, op[4]], pr.at[k, op[4]], op, key + ("pr",), "d").start()
            elif what == "l0":
                remote(sb.at[k, 1, lower], rl.at[k, 0], op, key + ("l0",), "x+").start()
            elif what == "l1":
                remote(sb.at[k, 1, upper], rl.at[k, 1], op, key + ("l1",), "x-").start()
            elif what == "ra1":
                remote(sb.at[k, 0, upper], ra.at[k, upper], op, key + ("ra",), "x+").start()
            elif what == "rb0":
                remote(sb.at[k, 2, lower], rb.at[k, lower], op, key + ("rb",), "x-").start()
            elif what == "ra0":
                remote(tt.at[k, 0], ra.at[k, lower], op, key + ("ra",), "x+").start()
            elif what == "rb1":
                remote(tt.at[k, 1], rb.at[k, upper], op, key + ("rb",), "x-").start()
            elif what == "yx":
                remote(yo.at[h - 2], yx.at[h - 2], op, ("rs", 0, h - 2, "yx"), "q").start()
        elif kind == "all":
            if op[1] == "w":
                name = op[2]
                for part in parts_of(name):
                    many = last_ones(part)[0] * rows_of(name, part)
                    wait_for(g[name].at[pl.ds(0, many)], ("all", name, part))
            elif op[1] == "ag":
                wait_for(xg.at[op[2], pl.ds(0, 4), pl.ds(0, ROWS)], op[1:])
            else:
                _, _, s, h, what = op
                k = slot(s, h)
                at = {"pr": pr.at[k], "l0": rl.at[k, 0], "l1": rl.at[k, 1], "ra": ra.at[k], "rb": rb.at[k], "yx": yx.at[h % 2]}
                wait_for(at[what], op[1:])
        else:
            what, s, h = op[1:4]
            k = slot(s, h)
            if what == "norm":
                norm(s, h)
            elif what == "gu":
                gate_up(s, h, op[4])
            elif what == "mix":
                mix(h)
            elif what == "down":
                down(s, h, op[4], op[5])
            elif what == "pair":
                po[h, 0] = po[h, 0] + pr[k, 0].astype(F32)
                for r in (2, 1, 3):
                    sb[k, r - 1] = (po[h, r] + pr[k, r].astype(F32)).astype(BF16)
            elif what == "relay0":
                tt[k, 0] = (sb[k, 0, :HALF].astype(F32) + rl[k, 0].astype(F32)).astype(BF16)
            elif what == "relay1":
                tt[k, 1] = (sb[k, 2, HALF:].astype(F32) + rl[k, 1].astype(F32)).astype(BF16)
            else:
                total = po[h, 0] + ra[k].astype(F32) + rb[k].astype(F32)
                if what == "give":
                    yo[h - 2] = total.astype(BF16)
                    continue
                if s == 0:
                    total = total + yx[h].astype(F32)
                at = slice(h * ROWS, (h + 1) * ROWS)
                value = (xg[s, tp, at].astype(F32) + (1.0 if s == 1 else 0.5) * total).astype(BF16)
                if s < 2:
                    xg[s + 1, tp, at] = value
                else:
                    out[at, :] = value

    for name in NAMES:
        for part in parts_of(name):
            wait_for(g[name].at[pl.ds(0, last_ones(part)[1] * rows_of(name, part))], ("sent", name, part))
    for op in plan()[0]:
        if op[0] == "pass":
            ref = block_at(op[1], op[2], op[3])
            if op[3] in ("m1", "p1") and op[4] != "d":
                ref = ref.at[lower]
            wait_for(ref, op)
        elif op[0] == "rsend":
            wait_for(ps.at[0, 0] if op[1] in ("pr", "yx") else rl.at[0, 0], op)
        elif op[0] == "swap":
            wait_for(ps.at[0, 0], op)


def body(resid, norm_gains, gate_one, up_one, down_one, proj_u, proj_v, spatial, spatial_bias, mix_gain, head_gain, proj_out, gate_two, up_two, down_two):
    weights = (gate_one, up_one, down_one.T, proj_u, proj_v, proj_out.T, gate_two, up_two, down_two.T)
    small = (norm_gains, spatial, spatial_bias, mix_gain.reshape(1, 128), head_gain.reshape(1, 128))
    raw = (gate_one, up_one, down_one.T, gate_two, up_two, down_two.T)
    sems_of = semaphores()
    rows, width = resid.shape
    return pl.pallas_call(
        functools.partial(kernel, sems_of),
        out_shape=jax.ShapeDtypeStruct((rows, width), BF16),
        in_specs=[pl.BlockSpec(memory_space=pltpu.HBM)] * 15,
        out_specs=pl.BlockSpec(memory_space=pltpu.VMEM),
        scratch_shapes=[pltpu.VMEM((2048, ITEMS[name][0]), BF16) for name in NAMES]
        + [pltpu.VMEM((2048, ITEMS[name][0]), BF16) for name in SPLIT]
        + [
            pltpu.VMEM((4, 8, 256, 256), BF16),
            pltpu.VMEM((STREAMS, ROWS, 2048), BF16),
            pltpu.VMEM((STREAMS, ROWS, 768), BF16),
            pltpu.VMEM((8, 4, ROWS, 256), BF16),
            pltpu.VMEM((8, 4, ROWS, 256), BF16),
            pltpu.VMEM((STREAMS, 4, ROWS, 256), F32),
            pltpu.VMEM((8, 3, ROWS, 256), BF16),
            pltpu.VMEM((8, 2, HALF, 256), BF16),
            pltpu.VMEM((8, ROWS, 256), BF16),
            pltpu.VMEM((8, ROWS, 256), BF16),
            pltpu.VMEM((8, 2, HALF, 256), BF16),
            pltpu.VMEM((2, ROWS, 256), BF16),
            pltpu.VMEM((2, ROWS, 256), BF16),
        ]
        + [pltpu.VMEM(a.shape, a.dtype) for a in raw + small]
        + [pltpu.SemaphoreType.DMA((25,)), pltpu.SemaphoreType.DMA((len(sems_of),))],
        compiler_params=pltpu.CompilerParams(collective_id=0, has_side_effects=True, vmem_limit_bytes=60 * 2**20),
        name="layer",
    )(*weights, resid, *small)


def solution(mesh):
    in_specs = (
        P(("rep", "fs"), "tp"),
        P(),
        P("fs", "tp"),
        P("fs", "tp"),
        P("tp", "fs"),
        P("fs", "tp"),
        P("fs", "tp"),
        P("tp", None, None),
        P("tp", None),
        P("tp"),
        P("tp"),
        P("tp", "fs"),
        P("fs", "tp"),
        P("fs", "tp"),
        P("tp", "fs"),
    )
    return jax.shard_map(body, mesh=mesh, in_specs=in_specs, out_specs=P(("rep", "fs"), "tp"), check_vma=False)
```

```python
import functools
import heapq

import jax
import jax.numpy as jnp
from jax import lax
from jax.experimental import pallas as pl
from jax.experimental.pallas import tpu as pltpu
from jax.sharding import PartitionSpec as P

MESH = pl.DeviceIdType.MESH
BF16, F32 = jnp.bfloat16, jnp.float32
SHARD = 64
ITEMS = {
    "f1": (1152, 48),
    "m": (512, 48),
    "f2a": (1024, 32),
    "f2b": (1024, 48),
}
NAMES = tuple(ITEMS)
SPLIT = ("f1",)
TURN = {"f1": 0, "m": 1, "f2a": 2, "f2b": 2}
RATE = {"y+": 46600.0, "y-": 46600.0, "z+": 46600.0, "z-": 46600.0, "x+": 46600.0, "x-": 46600.0, "d": 250000.0, "q": 30000.0}
DELAY = {"d": 1.5}
GREET = ("y+", "y-", "z+", "z-", "x+", "x-", "d")
AHEAD = 2.0
LEAST = 0.5
ROWS = 128
HALF = 64
BLOCK_BYTES = ROWS * 256 * 2
STREAMS = 4
Y_FIRST, Z_FIRST, Y_SAME, Y_CROSS, Z_SAME, Z_CROSS = range(6)
TWICE_UP = (-3, -1, 1, 3)


def parts_of(name):
    return (Y_SAME, Y_CROSS, Z_SAME, Z_CROSS) if name in SPLIT else (Y_FIRST, Z_FIRST)


def y_first(part):
    return part in (Y_FIRST, Y_SAME, Y_CROSS)


def rows_of(name, part):
    return ITEMS[name][1] if y_first(part) else SHARD - ITEMS[name][1]


def needed(part, dy):
    return part in (Y_FIRST, Z_FIRST) or (dy % 2 == 0) == (part in (Y_SAME, Z_SAME))


def reach(part, dz):
    if part in (Y_SAME, Z_SAME):
        return (4, 2) if dz in (0, 2) else (2, 4)
    if part in (Y_CROSS, Z_CROSS):
        return 3, 3
    return (4, 3) if y_first(part) or dz == 2 else (3, 4)


def children(part, dy, dz):
    out = []
    up, down = reach(part, dz)
    if y_first(part):
        if dz == 0:
            if 0 <= dy < up:
                out.append(("y+", dy + 1, 0))
            if -down < dy <= 0:
                out.append(("y-", dy - 1, 0))
            if needed(part, dy):
                out += [("z+", dy, 1), ("z-", dy, -1)]
        elif dz == 1 and dy in UP[part]:
            out.append(("z+", dy, 2))
        elif dz == -1 and dy not in UP[part]:
            out.append(("z-", dy, -2))
    elif dy == 0:
        if dz == 0:
            out += [("z+", 0, 1), ("z-", 0, -1)]
        elif dz == 1 and part != Z_CROSS:
            out.append(("z+", 0, 2))
        elif dz == -1 and part == Z_CROSS:
            out.append(("z-", 0, -2))
        out += [("y+", 1, dz), ("y-", -1, dz)]
    elif 0 < dy < up:
        out.append(("y+", dy + 1, dz))
    elif -down < dy < 0:
        out.append(("y-", dy - 1, dz))
    return out


UP = {Y_FIRST: (-3, -1, 1, 3), Y_SAME: (0, 4), Y_CROSS: (-1, 1)}


def last_ones(part):
    ends = total = 0
    todo = [(0, 0)]
    while todo:
        here = todo.pop()
        after = children(part, *here)
        ends += not after
        total += 1
        todo += [(a, b) for _, a, b in after]
    return ends, total - 1


def depth(part, dy, dz):
    return max((1 + depth(part, a, b) for _, a, b in children(part, dy, dz)), default=0)


def gather_steps():
    block, half = BLOCK_BYTES, BLOCK_BYTES // 2
    return {
        "own": [("x+", block, "m1"), ("x-", block, "p1"), ("d", block, "end")],
        "m1": [("x+", half, "h0"), ("d", block, "end")],
        "p1": [("x-", half, "h1"), ("d", block, "end")],
        "h0": [("d", half, "end")],
        "h1": [("d", half, "end")],
    }


def chain(h):
    half = BLOCK_BYTES // 2
    steps = []
    for s in range(3 if h < 2 else 1):
        steps.append((("norm", s, h), [("ag", s, h)], 0.35, []))
        if s == 1:
            steps.append((("mix", s, h), [("w", "m")], 0.7, []))
        elif s == 0:
            steps.append((("gu", s, h, 0), [("w", "f1")], 0.5, []))
        else:
            for j in range(3):
                steps.append((("gu", s, h, j), [("w", "f2a"), ("w", "f2b")], 0.3, []))
        needs = [[("w", "f1")], [("w", "m")], [("w", "m"), ("w", "f2b")]][s]
        for r in (2, 1, 3, 0):
            steps.append((("down", s, h, r, 1), needs, 0.1, [("d", BLOCK_BYTES, ("rs", s, h, "pr"), ("pr", s, h, r))]))
        for r in (2, 1, 3, 0):
            steps.append((("down", s, h, r, 0), [], 0.1, []))
        key = ("rs", s, h)
        steps.append(
            (
                ("pair", s, h),
                [key + ("pr",)],
                0.25,
                [
                    ("x+", half, key + ("l0",), ("l0", s, h)),
                    ("x-", half, key + ("l1",), ("l1", s, h)),
                    ("x+", half, key + ("ra",), ("ra1", s, h)),
                    ("x-", half, key + ("rb",), ("rb0", s, h)),
                ],
            )
        )
        steps.append((("relay0", s, h), [key + ("l0",)], 0.1, [("x+", half, key + ("ra",), ("ra0", s, h))]))
        steps.append((("relay1", s, h), [key + ("l1",)], 0.1, [("x-", half, key + ("rb",), ("rb1", s, h))]))
        waits = [key + ("ra",), key + ("rb",)]
        if h >= 2:
            steps.append((("give", s, h), waits, 0.15, [("q", BLOCK_BYTES, ("rs", 0, h - 2, "yx"), ("yx", s, h))]))
        else:
            steps.append((("end", s, h), waits + ([key + ("yx",)] if s == 0 else []), 0.2, [("next", s)]))
    return steps


SLOTS = [(s, h) for s in range(3) for h in range(2)] + [(0, 2), (0, 3)]


@functools.lru_cache(None)
def plan():
    count = {("w", name, part): last_ones(part)[0] for name in NAMES for part in parts_of(name)}
    expected = {}
    for s, h in SLOTS:
            expected[("ag", s, h)] = 5
            expected[("rs", s, h, "yx")] = 1
            expected[("rs", s, h, "pr")] = 4
            expected[("rs", s, h, "l0")] = expected[("rs", s, h, "l1")] = 1
            expected[("rs", s, h, "ra")] = expected[("rs", s, h, "rb")] = 2
    ops, now, serial = [], 0.0, 0
    free = {link: 0.0 for link in RATE}
    ready = {link: [] for link in RATE}
    arrivals, waited = [], set()

    def offer(link, priority, size, landing, op):
        nonlocal serial
        serial += 1
        heapq.heappush(ready[link], (priority, serial, size, landing, op))

    def offer_weight(index, name, part, dy, dz):
        for link, a, b in children(part, dy, dz):
            offer(
                link,
                (index, -depth(part, a, b)),
                rows_of(name, part) * ITEMS[name][0] * 2,
                ("w", index, name, part, a, b),
                ("send", name, part, dy, dz, link, a, b),
            )

    def offer_block(s, h, at):
        for link, size, landing in gather_steps()[at]:
            offer(link, (h, s), size, ("ag", s, h, landing), ("pass", s, h, at, link))

    def pump():
        nonlocal serial
        for link, queue in ready.items():
            while queue and free[link] - now < AHEAD:
                _, _, size, landing, op = heapq.heappop(queue)
                free[link] = max(free[link], now) + max(size / RATE[link], LEAST)
                if link == "q":
                    for shared in ("y+", "y-"):
                        free[shared] = max(free[shared], now) + 0.5 * size / RATE[shared]
                serial += 1
                heapq.heappush(arrivals, (free[link] + DELAY.get(link, 2.3), serial, landing))
                ops.append(op)

    for name in NAMES:
        for part in parts_of(name):
            offer_weight(TURN[name], name, part, 0, 0)
    for h in range(2):
        offer("q", (0, h), BLOCK_BYTES, ("ag", 0, h + 2, "own"), ("swap", h))
        offer_block(0, h, "own")
    chains = {h: chain(h) for h in (2, 3, 0, 1)}
    times = {}
    while any(chains.values()) or arrivals or any(ready.values()):
        while arrivals and arrivals[0][0] <= now:
            _, _, landing = heapq.heappop(arrivals)
            if landing[0] == "w":
                _, index, name, part, dy, dz = landing
                if children(part, dy, dz):
                    ops.append(("got", name, part, dy, dz))
                    offer_weight(index, name, part, dy, dz)
                else:
                    count[("w", name, part)] -= 1
            elif landing[0] == "ag" and landing[3] != "end":
                ops.append(("block",) + landing[1:])
                offer_block(*landing[1:])
            else:
                key = landing[:3] if landing[0] == "ag" else landing
                expected[key] -= 1
            times[landing[:3]] = now
        pump()
        ran = False
        for h, todo in chains.items():
            if not todo:
                continue
            step, needs, duration, sends = todo[0]
            done = True
            for need in needs:
                if need[0] == "w":
                    done &= all(count[("w", need[1], part)] == 0 for part in parts_of(need[1]))
                else:
                    done &= expected[need] == 0
            if not done:
                continue
            for need in needs:
                if need not in waited:
                    waited.add(need)
                    ops.append(("all",) + need)
            ops.append(("do",) + step)
            times[step] = now
            now += 0.6 * duration
            todo.pop(0)
            for send in sends:
                if send[0] == "next":
                    if send[1] < 2:
                        offer_block(send[1] + 1, h, "own")
                else:
                    offer(send[0], (-1, 0), send[1], send[2], ("rsend",) + send[3])
            ran = True
            break
        if ran:
            continue
        later = [arrivals[0][0]] if arrivals else []
        later += [free[link] - AHEAD + 0.01 for link, queue in ready.items() if queue]
        if not later:
            break
        now = max(min(later), now + 0.01)
    return ops, times, now


def semaphores():
    index = {}
    for name in NAMES:
        for part in parts_of(name):
            index[("all", name, part)] = len(index)
            index[("sent", name, part)] = len(index)
    for op in plan()[0]:
        if op[0] == "got":
            index[op[1:]] = len(index)
        elif op[0] in ("block", "pass", "rsend", "swap"):
            index[op] = len(index)
    for s, h in SLOTS:
        index[("ag", s, h)] = len(index)
        for what in ("pr", "l0", "l1", "ra", "rb", "yx"):
            index[("rs", s, h, what)] = len(index)
    return index


def rms_scale(values, mean_square, gain):
    return values * lax.rsqrt(mean_square + 1e-06) * gain


def contract(left, right):
    return lax.dot_general(left, right, (((1,), (1,)), ((), ())), preferred_element_type=F32)


def kernel(sems_of, *refs):
    gate_one, up_one, down_one, proj_u, proj_v, proj_out, gate_two, up_two, down_two = refs[:9]
    resid, small_in, out = refs[9], refs[10:15], refs[15]
    g = dict(zip(NAMES, refs[16:20]))
    passing = {"f1": refs[20]}
    (xg, normed, hidden, ps, pr, po, sb, rl, ra, rb, tt, yx, yo) = refs[21:34]
    raw, small, local_sem, sems = refs[34:40], refs[40:45], refs[45], refs[46]
    gains, spatial, bias, mix_gain, head_gain = small

    rep, fs, tp = lax.axis_index("rep"), lax.axis_index("fs"), lax.axis_index("tp")
    x, core = tp // 2, tp % 2
    y, z = fs % 8, rep * 4 + fs // 8
    odd = y % 2

    def device(link):
        if link[0] == "y":
            ny = (y + (1 if link[1] == "+" else 7)) % 8
            return {"rep": rep, "fs": (fs // 8) * 8 + ny, "tp": tp}
        if link[0] == "z":
            nz = (z + (1 if link[1] == "+" else 7)) % 8
            return {"rep": nz // 4, "fs": (nz % 4) * 8 + y, "tp": tp}
        if link[0] == "x":
            nx = (x + (1 if link[1] == "+" else 3)) % 4
            return {"rep": rep, "fs": fs, "tp": nx * 2 + core}
        if link == "q":
            return {"rep": rep, "fs": fs + 1 - 2 * odd, "tp": tp}
        return {"rep": rep, "fs": fs, "tp": x * 2 + 1 - core}

    devices = {link: device(link) for link in RATE}
    barrier = pltpu.get_barrier_semaphore()
    for link in GREET:
        pl.semaphore_signal(barrier, inc=1, device_id=devices[link], device_id_type=MESH)

    own = pl.multiple_of(fs * SHARD, SHARD)
    rows = pl.ds(own, SHARD)
    early = [(resid, xg.at[0, tp])] + list(zip((gate_one, up_one, down_one), raw[:3]))
    for array, side in ((g["f1"], odd), (passing["f1"], 1 - odd)):
        main = pl.ds(pl.multiple_of(side * 256, 256), 256)
        early += [(w.at[:, main], array.at[rows, pl.ds(384 * k, 256)]) for k, w in enumerate((gate_one, up_one, down_one))]
    late = list(zip((gate_two, up_two, down_two), raw[3:])) + [
        (proj_u, g["m"].at[rows, pl.ds(0, 128)]),
        (proj_v, g["m"].at[rows, pl.ds(128, 128)]),
        (proj_out, g["m"].at[rows, pl.ds(256, 128)]),
        (gate_two.at[:, pl.ds(0, 640)], g["f2a"].at[rows, pl.ds(0, 640)]),
        (down_two.at[:, pl.ds(0, 256)], g["f2a"].at[rows, pl.ds(768, 256)]),
        (up_two.at[:, pl.ds(0, 640)], g["f2b"].at[rows, pl.ds(0, 640)]),
        (down_two.at[:, pl.ds(256, 384)], g["f2b"].at[rows, pl.ds(640, 384)]),
    ]
    late += list(zip(small_in, small))
    copies = [pltpu.make_async_copy(src, dst, local_sem.at[k]) for k, (src, dst) in enumerate(early + late)]
    for copy in copies:
        copy.start()
    empty = jnp.zeros((SHARD, 64), BF16)
    for copy in copies[: len(early)]:
        copy.wait()
    for k in range(3):
        low = raw[k][:, 512:640]
        high = jnp.concatenate([raw[k][:, 640:704], empty], axis=1)
        column = 384 * k + 256
        g["f1"][rows, column : column + 128] = jnp.where(odd == 0, low, high)
        passing["f1"][rows, column : column + 128] = jnp.where(odd == 0, high, low)
    pl.semaphore_wait(barrier, len(GREET))

    def prepare_rest():
        for copy in copies[len(early) :]:
            copy.wait()
        g["f2a"][rows, 640:768] = jnp.concatenate([raw[4][:, 640:704], raw[3][:, 640:704]], axis=1)
        g["m"][rows, 384:512] = jnp.concatenate([empty, raw[5][:, 640:704]], axis=1)

    def piece(name, part, dy, dz, at=None):
        f = ((z + 8 - dz) % 4) * 8 + (y + 8 - dy) % 8
        start = f * SHARD + (0 if y_first(part) else ITEMS[name][1])
        array = g[name] if needed(part, dy if at is None else at) else passing[name]
        return array.at[pl.ds(pl.multiple_of(start, 16), rows_of(name, part))]

    def remote(src, dst, send, recv, link):
        return pltpu.make_async_remote_copy(
            src_ref=src,
            dst_ref=dst,
            send_sem=sems.at[sems_of[send]],
            recv_sem=sems.at[sems_of[recv]],
            device_id=devices[link],
            device_id_type=MESH,
        )

    def wait_for(ref, key):
        pltpu.make_async_copy(ref, ref, sems.at[sems_of[key]]).wait()

    def block_at(s, h, at):
        shift = {"own": 0, "m1": 3, "p1": 1, "h0": 2, "h1": 2}[at]
        start, size = (h % 2) * ROWS, ROWS
        if at[0] == "h":
            start, size = start + (0 if at == "h0" else HALF), HALF
        return xg.at[3 if h >= 2 else s, ((x + shift) % 4) * 2 + core, pl.ds(start, size)]

    def slot(s, h):
        return SLOTS.index((s, h))

    def down(s, h, r, other):
        t = ((x + r) % 4) * 2 + (1 - core if other else core)
        at = pl.ds(pl.multiple_of(t * 256, 256), 256)
        if s == 1:
            total = contract(hidden[h, :, :128], g["m"][at, 256:384])
        elif s == 0:
            total = contract(hidden[h, :, :384], g["f1"][at, 768:1152])
        else:
            total = contract(hidden[h, :, :256], g["f2a"][at, 768:1024])
            total = total + contract(hidden[h, :, 256:640], g["f2b"][at, 640:1024])
            total = total + contract(hidden[h, :, 640:768], g["m"][at, 384:512])
        if other:
            ps[slot(s, h), r] = total.astype(BF16)
        else:
            po[h, r] = total

    def gate_up(s, h, j):
        if s == 0:
            gate = jnp.dot(normed[h], g["f1"][:, 0:384], preferred_element_type=F32)
            up = jnp.dot(normed[h], g["f1"][:, 384:768], preferred_element_type=F32)
            hidden[h, :, :384] = (jax.nn.silu(gate) * up).astype(BF16)
            return
        a, b = g["f2a"], g["f2b"]
        first = jnp.dot(normed[h], a[:, 256 * j : 256 * (j + 1)], preferred_element_type=F32)
        if j < 2:
            second = jnp.dot(normed[h], b[:, 256 * j : 256 * (j + 1)], preferred_element_type=F32)
            hidden[h, :, 256 * j : 256 * (j + 1)] = (jax.nn.silu(first) * second).astype(BF16)
            return
        second = jnp.dot(normed[h], b[:, 512:640], preferred_element_type=F32)
        hidden[h, :, 512:640] = (jax.nn.silu(first[:, :128]) * second).astype(BF16)
        rest = first[:, 128:]
        value = jax.nn.silu(rest) * pltpu.roll(rest, 64, 1)
        lane = lax.broadcasted_iota(jnp.int32, (ROWS, 128), 1)
        hidden[h, :, 640:768] = jnp.where(lane >= 64, value, 0.0).astype(BF16)

    def norm(s, h):
        rows = slice((h % 2) * ROWS, (h % 2 + 1) * ROWS)
        stage, s = s, 3 if h >= 2 else s
        total = jnp.zeros((ROWS, 1), F32)
        for t in range(8):
            values = xg[s, t, rows].astype(F32)
            total = total + jnp.sum(values * values, axis=-1, keepdims=True)
        for t in range(8):
            cols = slice(256 * t, 256 * (t + 1))
            scaled = rms_scale(xg[s, t, rows].astype(F32), total / 2048.0, gains[stage : stage + 1, cols])
            normed[h, :, cols] = scaled.astype(BF16)

    def mix(h):
        both = jnp.dot(normed[h], g["m"][:, 0:256], preferred_element_type=F32)
        u, v = jax.nn.gelu(both[:, :128]), jax.nn.gelu(both[:, 128:])
        centre = jnp.mean(v, axis=-1, keepdims=True)
        spread = jnp.mean(jnp.square(v - centre), axis=-1, keepdims=True)
        vn = ((v - centre) * lax.rsqrt(spread + 1e-05) * mix_gain[...]).astype(BF16)
        to, source = lax.broadcasted_iota(jnp.int32, (128, 128), 0), lax.broadcasted_iota(jnp.int32, (128, 128), 1)
        masked = jnp.where(to // 64 >= source // 64, spatial[0].astype(F32), 0.0).astype(BF16)
        offset = jnp.sum(jnp.where(to == source, bias[...], 0.0), axis=-1, keepdims=True)
        product = u * (jnp.dot(masked, vn, preferred_element_type=F32) + offset)
        square = jnp.mean(product * product, axis=-1, keepdims=True)
        hidden[h, :, :128] = rms_scale(product, square, head_gain[...]).astype(BF16)

    lower, upper = pl.ds(0, HALF), pl.ds(HALF, HALF)
    prepared = False
    for op in plan()[0]:
        kind = op[0]
        if not prepared and (kind == "got" or (kind == "send" and op[1] != "f1") or kind in ("all", "do")):
            prepared = True
            prepare_rest()
        if kind == "send":
            _, name, part, dy, dz, link, a, b = op
            landing = (name, part, a, b) if children(part, a, b) else ("all", name, part)
            remote(piece(name, part, dy, dz), piece(name, part, dy, dz, a), ("sent", name, part), landing, link).start()
        elif kind == "swap":
            h = op[1]
            src, dst = xg.at[0, tp, pl.ds(h * ROWS, ROWS)], xg.at[3, tp, pl.ds(h * ROWS, ROWS)]
            remote(src, dst, op, ("block", 0, h + 2, "own"), "q").start()
        elif kind == "got":
            _, name, part, dy, dz = op
            wait_for(piece(name, part, dy, dz), op[1:])
        elif kind == "pass":
            _, s, h, at, link = op
            ref = block_at(s, h, at)
            if link == "d":
                landing = ("ag", s, h)
            else:
                arrived = {"own": {"x+": "m1", "x-": "p1"}, "m1": {"x+": "h0"}, "p1": {"x-": "h1"}}[at][link]
                landing = ("block", s, h, arrived)
                if at == "m1":
                    ref = ref.at[lower]
                elif at == "p1":
                    ref = ref.at[upper]
            remote(ref, ref, op, landing, link).start()
        elif kind == "block":
            wait_for(block_at(*op[1:]), op)
        elif kind == "rsend":
            what, s, h = op[1:4]
            key, k = ("rs", s, h), slot(s, h)
            if what == "pr":
                remote(ps.at[k, op[4]], pr.at[k, op[4]], op, key + ("pr",), "d").start()
            elif what == "l0":
                remote(sb.at[k, 1, lower], rl.at[k, 0], op, key + ("l0",), "x+").start()
            elif what == "l1":
                remote(sb.at[k, 1, upper], rl.at[k, 1], op, key + ("l1",), "x-").start()
            elif what == "ra1":
                remote(sb.at[k, 0, upper], ra.at[k, upper], op, key + ("ra",), "x+").start()
            elif what == "rb0":
                remote(sb.at[k, 2, lower], rb.at[k, lower], op, key + ("rb",), "x-").start()
            elif what == "ra0":
                remote(tt.at[k, 0], ra.at[k, lower], op, key + ("ra",), "x+").start()
            elif what == "rb1":
                remote(tt.at[k, 1], rb.at[k, upper], op, key + ("rb",), "x-").start()
            elif what == "yx":
                remote(yo.at[h - 2], yx.at[h - 2], op, ("rs", 0, h - 2, "yx"), "q").start()
        elif kind == "all":
            if op[1] == "w":
                name = op[2]
                for part in parts_of(name):
                    many = last_ones(part)[0] * rows_of(name, part)
                    wait_for(g[name].at[pl.ds(0, many)], ("all", name, part))
            elif op[1] == "ag":
                wait_for(xg.at[op[2], pl.ds(0, 4), pl.ds(0, ROWS)], op[1:])
            else:
                _, _, s, h, what = op
                k = slot(s, h)
                at = {"pr": pr.at[k], "l0": rl.at[k, 0], "l1": rl.at[k, 1], "ra": ra.at[k], "rb": rb.at[k], "yx": yx.at[h % 2]}
                wait_for(at[what], op[1:])
        else:
            what, s, h = op[1:4]
            k = slot(s, h)
            if what == "norm":
                norm(s, h)
            elif what == "gu":
                gate_up(s, h, op[4])
            elif what == "mix":
                mix(h)
            elif what == "down":
                down(s, h, op[4], op[5])
            elif what == "pair":
                po[h, 0] = po[h, 0] + pr[k, 0].astype(F32)
                for r in (2, 1, 3):
                    sb[k, r - 1] = (po[h, r] + pr[k, r].astype(F32)).astype(BF16)
            elif what == "relay0":
                tt[k, 0] = (sb[k, 0, :HALF].astype(F32) + rl[k, 0].astype(F32)).astype(BF16)
            elif what == "relay1":
                tt[k, 1] = (sb[k, 2, HALF:].astype(F32) + rl[k, 1].astype(F32)).astype(BF16)
            else:
                total = po[h, 0] + ra[k].astype(F32) + rb[k].astype(F32)
                if what == "give":
                    yo[h - 2] = total.astype(BF16)
                    continue
                if s == 0:
                    total = total + yx[h].astype(F32)
                at = slice(h * ROWS, (h + 1) * ROWS)
                value = (xg[s, tp, at].astype(F32) + (1.0 if s == 1 else 0.5) * total).astype(BF16)
                if s < 2:
                    xg[s + 1, tp, at] = value
                else:
                    out[at, :] = value

    for name in NAMES:
        for part in parts_of(name):
            wait_for(g[name].at[pl.ds(0, last_ones(part)[1] * rows_of(name, part))], ("sent", name, part))
    for op in plan()[0]:
        if op[0] == "pass":
            ref = block_at(op[1], op[2], op[3])
            if op[3] in ("m1", "p1") and op[4] != "d":
                ref = ref.at[lower]
            wait_for(ref, op)
        elif op[0] == "rsend":
            wait_for(ps.at[0, 0] if op[1] in ("pr", "yx") else rl.at[0, 0], op)
        elif op[0] == "swap":
            wait_for(ps.at[0, 0], op)


def body(resid, norm_gains, gate_one, up_one, down_one, proj_u, proj_v, spatial, spatial_bias, mix_gain, head_gain, proj_out, gate_two, up_two, down_two):
    weights = (gate_one, up_one, down_one.T, proj_u, proj_v, proj_out.T, gate_two, up_two, down_two.T)
    small = (norm_gains, spatial, spatial_bias, mix_gain.reshape(1, 128), head_gain.reshape(1, 128))
    raw = (gate_one, up_one, down_one.T, gate_two, up_two, down_two.T)
    sems_of = semaphores()
    rows, width = resid.shape
    return pl.pallas_call(
        functools.partial(kernel, sems_of),
        out_shape=jax.ShapeDtypeStruct((rows, width), BF16),
        in_specs=[pl.BlockSpec(memory_space=pltpu.HBM)] * 15,
        out_specs=pl.BlockSpec(memory_space=pltpu.VMEM),
        scratch_shapes=[pltpu.VMEM((2048, ITEMS[name][0]), BF16) for name in NAMES]
        + [pltpu.VMEM((2048, ITEMS[name][0]), BF16) for name in SPLIT]
        + [
            pltpu.VMEM((4, 8, 256, 256), BF16),
            pltpu.VMEM((STREAMS, ROWS, 2048), BF16),
            pltpu.VMEM((STREAMS, ROWS, 768), BF16),
            pltpu.VMEM((8, 4, ROWS, 256), BF16),
            pltpu.VMEM((8, 4, ROWS, 256), BF16),
            pltpu.VMEM((STREAMS, 4, ROWS, 256), F32),
            pltpu.VMEM((8, 3, ROWS, 256), BF16),
            pltpu.VMEM((8, 2, HALF, 256), BF16),
            pltpu.VMEM((8, ROWS, 256), BF16),
            pltpu.VMEM((8, ROWS, 256), BF16),
            pltpu.VMEM((8, 2, HALF, 256), BF16),
            pltpu.VMEM((2, ROWS, 256), BF16),
            pltpu.VMEM((2, ROWS, 256), BF16),
        ]
        + [pltpu.VMEM(a.shape, a.dtype) for a in raw + small]
        + [pltpu.SemaphoreType.DMA((25,)), pltpu.SemaphoreType.DMA((len(sems_of),))],
        compiler_params=pltpu.CompilerParams(collective_id=0, has_side_effects=True, vmem_limit_bytes=60 * 2**20),
        name="layer",
    )(*weights, resid, *small)


def solution(mesh):
    in_specs = (
        P(("rep", "fs"), "tp"),
        P(),
        P("fs", "tp"),
        P("fs", "tp"),
        P("tp", "fs"),
        P("fs", "tp"),
        P("fs", "tp"),
        P("tp", None, None),
        P("tp", None),
        P("tp"),
        P("tp"),
        P("tp", "fs"),
        P("fs", "tp"),
        P("fs", "tp"),
        P("tp", "fs"),
    )
    return jax.shard_map(body, mesh=mesh, in_specs=in_specs, out_specs=P(("rep", "fs"), "tp"), check_vma=False)
```
